512 devices in a mesh: rep: 2 (over z_hi), fs: 32 (over z_lo, y), tp: 8 (over x, core).
Axes of the slice: x: 4, y: 4, z: 16 (z_hi: 2, z_lo: 8; z = z_hi * 8 + z_lo), core: 2. Of those that a mesh axis runs over, the one named last changes fastest.
Arguments:
- stream: bfloat16 [24576, 2048], P(('rep', 'fs'), 'tp'), may hold values from -24 to 24
- recurrence_input_weight: bfloat16 [2048, 2048], P('fs', 'tp'), may hold values from -0.125 to 0.125
- output_gate_weight: bfloat16 [2048, 2048], P('fs', 'tp'), may hold values from -0.125 to 0.125
- recurrence_gate_matrix: bfloat16 [16, 128, 128], P('tp'), may hold values from -0.5 to 0.5
- input_gate_matrix: bfloat16 [16, 128, 128], P('tp'), may hold values from -0.5 to 0.5
- channel_decay_rate: float32 [2048], P('tp')
- recurrence_taps: float32 [4, 2048], P(None, 'tp'), may hold values from -3 to 3
- spike_log_decay: float32 [24576, 16], P(('rep', 'fs'), 'tp'), may hold values from -2.1 to 0
- recurrence_output_weight: bfloat16 [2048, 2048], P('tp', 'fs'), may hold values from -0.3125 to 0.3125
- feedforward_gate_upward: bfloat16 [2048, 4096], P('fs', 'tp'), may hold values from -0.125 to 0.125
- feedforward_value_upward: bfloat16 [2048, 4096], P('fs', 'tp'), may hold values from -0.125 to 0.125
- feedforward_gate_taps: float32 [3, 4096], P(None, 'tp'), may hold values from -3 to 3
- feedforward_value_taps: float32 [3, 4096], P(None, 'tp'), may hold values from -3 to 3
- feedforward_down_weight: bfloat16 [4096, 2048], P('tp', 'fs'), may hold values from -0.1875 to 0.1875
- recurrence_norm_gain: float32 [2048], replicated, may hold values from 0.1 to 1.9
- feedforward_norm_gain: float32 [2048], replicated, may hold values from 0.1 to 1.9
- closing_norm_gain: float32 [2048], replicated, may hold values from 0.1 to 1.9
Outputs:
- layer_out: bfloat16 [24576, 2048], P(('rep', 'fs'), 'tp')
The draws below stay inside these ranges and needn't reach their ends.
All inputs are finite; a program needn't handle non-finite values.
Results may differ from the reference program's by a relative error of at most 0.018.
Values may be sent and summed in bfloat16 or wider, within the bound.
A program may use at most 64 MiB of HBM per device.

```python
import math
import jax
import jax.numpy as jnp
from jax import lax

MODEL_WIDTH = 2048
GATE_BLOCKS = 16
BLOCK = 128
R = 2048
FF = 4096
CONV = 4
FCONV = 3
SEQUENCE_TOKENS = 384
TOKEN_TOTAL = 24576
N_TP = 8


def draw_stream(key, part):
    row_key, sample_key = jax.random.split(jax.random.fold_in(key, 11), 2)
    samples = jax.random.truncated_normal(sample_key, -4.0, 4.0, (TOKEN_TOTAL, MODEL_WIDTH), jnp.float32)
    column_scale = jnp.exp(math.log(3.0) * jnp.arange(MODEL_WIDTH, dtype=jnp.float32) / MODEL_WIDTH)
    row_scale = jnp.exp(jax.random.uniform(row_key, (TOKEN_TOTAL, 1), jnp.float32, math.log(0.5), math.log(2.0)))
    return (samples * row_scale * column_scale[None, :]).astype(jnp.bfloat16)


def draw_channel_decay_rate(key, part):
    order_key, slow_key, fast_key = jax.random.split(jax.random.fold_in(key, 23), 3)
    ranking = jax.random.permutation(order_key, GATE_BLOCKS)
    slow_heads = ranking < GATE_BLOCKS // 2
    slow_rate = jnp.exp(jax.random.uniform(slow_key, (R,), jnp.float32, math.log(0.05), math.log(0.25))) / SEQUENCE_TOKENS
    fast_rate = jnp.exp(jax.random.uniform(fast_key, (R,), jnp.float32, math.log(0.006), math.log(0.025)))
    slow_mask = jnp.repeat(slow_heads, BLOCK)
    rate_per_step = jnp.where(slow_mask, slow_rate, fast_rate)
    return -jnp.log(jnp.expm1(rate_per_step))


def draw_spike_log_decay(key, part):
    position_random_key, depth_random_key = jax.random.split(jax.random.fold_in(key, 37), 2)
    sequence_count = TOKEN_TOTAL // SEQUENCE_TOKENS
    spike_positions = jax.random.randint(position_random_key, (sequence_count, 3, GATE_BLOCKS), 0, SEQUENCE_TOKENS)
    lower_limit = 0.5
    upper_limit = 0.8
    spike_depth = jnp.log(jax.random.uniform(depth_random_key, (sequence_count, 3, GATE_BLOCKS), jnp.float32, lower_limit, upper_limit))
    token_positions = jnp.arange(SEQUENCE_TOKENS)
    spike_hits = token_positions[None, None, :, None] == spike_positions[:, :, None, :]
    spike_total = jnp.sum(jnp.where(spike_hits, spike_depth[:, :, None, :], 0.0), axis=1)
    return spike_total.reshape(TOKEN_TOTAL, GATE_BLOCKS).astype(jnp.float32)


def steps_of(key, dims, shards, smallest, largest):
    factor_of = 1.0
    for dim, shards_of in shards:
        draws = jax.random.uniform(jax.random.fold_in(jax.random.fold_in(key, 6), dim), (shards_of,), jnp.float32, smallest / len(shards), largest / len(shards))
        factor_of = factor_of * jnp.repeat(jnp.exp(draws), dims[dim] // shards_of).reshape((-1,) + (1,) * (len(dims) - 1 - dim))
    return factor_of


def scatter_about(own_key, shape, spread, limit, shards=(), kind=jnp.bfloat16):
    result = jax.random.normal(own_key, shape, jnp.float32) * spread
    if len(shards) > 0:
        result = steps_of(own_key, shape, shards, -0.22, 0.18) * result
    return jnp.clip(result, min=-limit, max=limit).astype(kind)


def setup_inputs(seed: int = 0) -> dict:
    streams_of = jax.random.split(jax.random.key(seed), 18)
    stream = draw_stream(jax.random.fold_in(streams_of[17], 71), 0)
    recurrence_input_weight = scatter_about(streams_of[1], (MODEL_WIDTH, R), MODEL_WIDTH ** -0.5, 0.125, ((0, 32), (1, 8)))
    output_gate_weight = scatter_about(streams_of[2], (MODEL_WIDTH, R), MODEL_WIDTH ** -0.5, 0.125, ((0, 32), (1, 8)))
    recurrence_gate_matrix = scatter_about(streams_of[3], (GATE_BLOCKS, BLOCK, BLOCK), BLOCK ** -0.5, 0.5, ((0, 8),))
    input_gate_matrix = scatter_about(streams_of[4], (GATE_BLOCKS, BLOCK, BLOCK), BLOCK ** -0.5, 0.5, ((0, 8),))
    channel_decay_rate = draw_channel_decay_rate(jax.random.fold_in(streams_of[17], 71), 0)
    recurrence_taps = scatter_about(streams_of[6], (CONV, R), 0.5, 3.0, ((1, 8),), jnp.float32)
    spike_log_decay = draw_spike_log_decay(jax.random.fold_in(streams_of[17], 71), 0)
    recurrence_output_weight = scatter_about(streams_of[8], (R, MODEL_WIDTH), (R // 6) ** -0.5, 0.3125, ((0, 8), (1, 32)))
    feedforward_gate_upward = scatter_about(streams_of[9], (MODEL_WIDTH, FF), MODEL_WIDTH ** -0.5, 0.125, ((0, 32), (1, 8)))
    feedforward_value_upward = scatter_about(streams_of[10], (MODEL_WIDTH, FF), MODEL_WIDTH ** -0.5, 0.125, ((0, 32), (1, 8)))
    feedforward_gate_taps = scatter_about(streams_of[11], (FCONV, FF), 0.577, 3.0, ((1, 8),), jnp.float32)
    feedforward_value_taps = scatter_about(streams_of[12], (FCONV, FF), 0.577, 3.0, ((1, 8),), jnp.float32)
    feedforward_down_weight = scatter_about(streams_of[13], (FF, MODEL_WIDTH), (FF // 4) ** -0.5, 0.1875, ((0, 8), (1, 32)))
    recurrence_norm_gain = jnp.clip(1.0 + 0.18 * jax.random.normal(streams_of[14], (MODEL_WIDTH,), jnp.float32), 0.1, 1.9)
    feedforward_norm_gain = jnp.clip(1.0 + 0.18 * jax.random.normal(streams_of[15], (MODEL_WIDTH,), jnp.float32), 0.1, 1.9)
    closing_norm_gain = jnp.clip(1.0 + 0.18 * jax.random.normal(streams_of[16], (MODEL_WIDTH,), jnp.float32), 0.1, 1.9)
    return dict(stream=stream, recurrence_input_weight=recurrence_input_weight, output_gate_weight=output_gate_weight, recurrence_gate_matrix=recurrence_gate_matrix, input_gate_matrix=input_gate_matrix, channel_decay_rate=channel_decay_rate, recurrence_taps=recurrence_taps, spike_log_decay=spike_log_decay, recurrence_output_weight=recurrence_output_weight, feedforward_gate_upward=feedforward_gate_upward, feedforward_value_upward=feedforward_value_upward, feedforward_gate_taps=feedforward_gate_taps, feedforward_value_taps=feedforward_value_taps, feedforward_down_weight=feedforward_down_weight, recurrence_norm_gain=recurrence_norm_gain, feedforward_norm_gain=feedforward_norm_gain, closing_norm_gain=closing_norm_gain)


EPS = 1e-06
GATE_POWER = 8.0

def rms_scale(row_block, gain_vec):
    widened = row_block.astype(jnp.float32)
    inverse = lax.rsqrt(lax.optimization_barrier(jnp.mean(widened * widened, axis=-1, keepdims=True)) + EPS)
    return (widened * inverse * gain_vec).astype(jnp.bfloat16)

def causal_mix(values, kernel_taps):
    extent = kernel_taps.shape[0]
    length = values.shape[0]
    padded = jnp.pad(values, ((extent - 1, 0), (0, 0)))
    summed = kernel_taps[0] * padded[0:length]
    for offset in range(1, extent):
        summed = summed + kernel_taps[offset] * padded[offset:offset + length]
    return summed

def chain_step(earlier, following):
    return (earlier[0] * following[0], following[0] * earlier[1] + following[1])

def split_partials(left_rows, weight_rows, part_count):
    share_rows = left_rows.shape[1] // part_count
    summed = jnp.zeros((left_rows.shape[0], weight_rows.shape[1]), jnp.float32)
    for part_index in range(part_count):
        lower = part_index * share_rows
        partial_sum = jnp.dot(left_rows[:, lower:lower + share_rows], weight_rows[lower:lower + share_rows], preferred_element_type=jnp.float32).astype(jnp.bfloat16)
        summed = summed + lax.optimization_barrier(partial_sum).astype(jnp.float32)
    return summed

def reference(stream, recurrence_input_weight, output_gate_weight, recurrence_gate_matrix, input_gate_matrix, channel_decay_rate, recurrence_taps, spike_log_decay, recurrence_output_weight, feedforward_gate_upward, feedforward_value_upward, feedforward_gate_taps, feedforward_value_taps, feedforward_down_weight, recurrence_norm_gain, feedforward_norm_gain, closing_norm_gain):
    sequence_count = stream.shape[0] // SEQUENCE_TOKENS
    decay_base = (GATE_POWER * jax.nn.softplus(-channel_decay_rate)).reshape(GATE_BLOCKS, BLOCK)

    def single_sequence(input_rows):
        incoming_tokens, spike_events = input_rows
        normed = rms_scale(incoming_tokens, recurrence_norm_gain)
        rec_in = jnp.dot(normed, recurrence_input_weight, preferred_element_type=jnp.float32).astype(jnp.bfloat16)
        gate_src = jnp.dot(normed, output_gate_weight, preferred_element_type=jnp.float32).astype(jnp.bfloat16)
        conv_out = causal_mix(rec_in.astype(jnp.float32), recurrence_taps).astype(jnp.bfloat16)
        blocks = conv_out.astype(jnp.float32).reshape(SEQUENCE_TOKENS, GATE_BLOCKS, BLOCK)
        gate_restart = jax.nn.sigmoid(jnp.einsum('thi,hij->thj', blocks, recurrence_gate_matrix.astype(jnp.float32)))
        admit_gate = jax.nn.sigmoid(jnp.einsum('thi,hij->thj', blocks, input_gate_matrix.astype(jnp.float32)))
        decay_logarithm = -gate_restart * decay_base + spike_events[:, :, None]
        decay_rate = jnp.exp(decay_logarithm)
        inflow = jnp.sqrt(-jnp.expm1(2.0 * decay_logarithm)) * admit_gate * blocks
        states = lax.associative_scan(chain_step, (decay_rate, inflow), axis=0)[1]
        mixed_out = (states.reshape(SEQUENCE_TOKENS, R) * jax.nn.gelu(gate_src.astype(jnp.float32))).astype(jnp.bfloat16)
        branch = split_partials(mixed_out, recurrence_output_weight, N_TP).astype(jnp.bfloat16)
        middle = (incoming_tokens.astype(jnp.float32) + branch.astype(jnp.float32)).astype(jnp.bfloat16)
        normed_ffn = rms_scale(middle, feedforward_norm_gain)
        gate_up = jnp.dot(normed_ffn, feedforward_gate_upward, preferred_element_type=jnp.float32).astype(jnp.bfloat16)
        value_up = jnp.dot(normed_ffn, feedforward_value_upward, preferred_element_type=jnp.float32).astype(jnp.bfloat16)
        gate_conv = causal_mix(gate_up.astype(jnp.float32), feedforward_gate_taps)
        value_conv = causal_mix(value_up.astype(jnp.float32), feedforward_value_taps)
        hidden = (jax.nn.gelu(gate_conv) * value_conv).astype(jnp.bfloat16)
        branch_ffn = split_partials(hidden, feedforward_down_weight, N_TP).astype(jnp.bfloat16)
        final_rows = middle.astype(jnp.float32) + branch_ffn.astype(jnp.float32)
        inverse = lax.rsqrt(lax.optimization_barrier(jnp.mean(final_rows * final_rows, axis=-1, keepdims=True)) + EPS)
        return (final_rows * inverse * closing_norm_gain).astype(jnp.bfloat16)
    output_rows = lax.map(single_sequence, (stream.reshape(sequence_count, SEQUENCE_TOKENS, MODEL_WIDTH), spike_log_decay.reshape(sequence_count, SEQUENCE_TOKENS, GATE_BLOCKS)))
    return output_rows.reshape(sequence_count * SEQUENCE_TOKENS, MODEL_WIDTH)
```

```python
import functools

import jax
import jax.numpy as jnp
from jax import lax
from jax.experimental import pallas as pl
from jax.experimental.pallas import tpu as pltpu
from jax.sharding import PartitionSpec as P

EPS = 1e-06
GATE_POWER = 8.0
MESH = pl.DeviceIdType.MESH
NY, NZ, NX, NC = 4, 8, 4, 2
ZRING = 16
F32, BF16 = jnp.float32, jnp.bfloat16

FIRST_Y = (True, False, True, False, False, True)
LAGS = (0, 0, 1, 1, 2, 3)
LOG = []


class Net:
    def __init__(self, ssem, rsem):
        self.ssem, self.rsem = ssem, rsem
        self.count = 0
        self.started = []

    def send(self, src, dst, device, link):
        i = self.count
        self.count += 1
        copy = pltpu.make_async_remote_copy(
            src_ref=src, dst_ref=dst, send_sem=self.ssem.at[i], recv_sem=self.rsem.at[i],
            device_id=device, device_id_type=MESH,
        )
        copy.start()
        n = 1
        for s in src.shape:
            n *= s
        LOG.append(("start", link, n * src.dtype.itemsize, i))
        self.started.append(copy)
        copy.number = i
        return copy

    def arrived(self, copy):
        LOG.append(("wait", copy.number))
        copy.wait_recv()

    def drain(self):
        for copy in self.started:
            copy.wait_send()


def work(us):
    LOG.append(("work", us))


def sigmoid(v):
    return 1.0 / (1.0 + jnp.exp(-v))


def gelu(v):
    return 0.5 * v * (1.0 + jnp.tanh(0.7978845608028654 * (v + 0.044715 * (v * v * v))))


def softplus(v):
    t = jnp.exp(-jnp.abs(v))
    u = 1.0 + t
    small = u == 1.0
    log1p = jnp.where(small, t, jnp.log(u) * (t / jnp.where(small, 1.0, u - 1.0)))
    return jnp.maximum(v, 0.0) + log1p


def one_minus_exp(v):
    term = 1.0 + v * (1.0 / 9.0)
    for k in (8, 7, 6, 5, 4, 3, 2):
        term = 1.0 + v * (1.0 / k) * term
    return jnp.where(v > -0.5, -v * term, 1.0 - jnp.exp(v))


def nn(a, b):
    return lax.dot_general(a, b, (((1,), (0,)), ((), ())), preferred_element_type=F32)


def nt(a, b):
    return lax.dot_general(a, b, (((1,), (1,)), ((), ())), preferred_element_type=F32)


def layer_kernel(
    stream, w_in, w_gate, w_out, w_fg, w_fv, w_down,
    rgm, igm, rate, rtaps, spike, gtaps, vtaps, gain_r, gain_f, gain_c,
    out,
    g_in, g_gate, g_out, g_fg, g_fv, g_down,
    s_all, m_all, normed, pad_r, gate_src, mixed, pad_g, pad_v, hidden,
    own_sum, part_a, got_a, far_a, near_a, relay_a, fin_a,
    part_b, got_b, far_b, near_b, relay_b, fin_b,
    final, stats, ssem, rsem, lsem,
):
    rep, fs, tp = lax.axis_index("rep"), lax.axis_index("fs"), lax.axis_index("tp")
    zlo, y = fs // NY, fs % NY
    x, core = tp // NC, tp % NC
    z = rep * NZ + zlo
    zs = [(z + k) % ZRING for k in (1, ZRING - 1)]
    ys = [(y + k) % NY for k in (1, NY - 1)]
    xs = [(x + k) % NX for k in (1, NX - 1)]

    def at_z(zz):
        return {"rep": zz // NZ, "fs": (zz % NZ) * NY + y, "tp": tp}

    def at_y(yy):
        return {"rep": rep, "fs": zlo * NY + yy, "tp": tp}

    def at_x(xx, cc):
        return {"rep": rep, "fs": fs, "tp": xx * NC + cc}

    zup, zdn = at_z(zs[0]), at_z(zs[1])
    yup, ydn = at_y(ys[0]), at_y(ys[1])
    xup, xdn = at_x(xs[0], core), at_x(xs[1], core)
    pair = at_x(x, 1 - core)
    xfar = (x + 2) % NX

    shards = (w_in, w_gate, w_out, w_fg, w_fv, w_down)
    wholes = (g_in, g_gate, g_out, g_fg, g_fv, g_down)
    loads = [pltpu.make_async_copy(stream, s_all.at[tp], lsem.at[6])]
    for i in range(6):
        loads.append(pltpu.make_async_copy(shards[i], wholes[i].at[zlo, y], lsem.at[i]))
    for copy in loads:
        copy.start()

    others = [at_x(xx, cc) for xx in (xs[0], xs[1], xfar) for cc in (core, 1 - core)] + [pair]
    barrier = pltpu.get_barrier_semaphore()
    friends = [zup, zdn, yup, ydn] + others
    for friend in friends:
        pl.semaphore_signal(barrier, inc=1, device_id=friend, device_id_type=MESH)
    pl.semaphore_wait(barrier, len(friends))
    work(2.5)
    for copy in loads:
        copy.wait()

    net = Net(ssem, rsem)
    flight = [{} for _ in range(6)]

    def zslot(k):
        return (zlo + k + NZ) % NZ

    def yslot(k):
        return (y + k + NY) % NY

    def both(i, key, up_src, dn_src, up, dn, links):
        flight[i][key] = (net.send(up_src, up_src, up, links[0]), net.send(dn_src, dn_src, dn, links[1]))

    def landed(i, key):
        for copy in flight[i][key]:
            net.arrived(copy)

    def step(i, s):
        g = wholes[i]
        first_y = FIRST_Y[i]
        zl, yl = ("z+", "z-"), ("y+", "y-")
        if first_y:
            if s == 0:
                own = g.at[zlo, y]
                both(i, 0, own, own, yup, ydn, yl)
            elif s == 1:
                landed(i, 0)
                half = g.shape[2] // 2
                both(i, 1, g.at[zlo, yslot(-1), pl.ds(0, half)], g.at[zlo, yslot(1), pl.ds(half, half)], yup, ydn, yl)
            elif s == 2:
                landed(i, 1)
                both(i, 2, g.at[zlo], g.at[zlo], zup, zdn, zl)
            elif s in (3, 4):
                landed(i, s - 1)
                both(i, s, g.at[zslot(2 - s)], g.at[zslot(s - 2)], zup, zdn, zl)
            elif s == 5:
                landed(i, 4)
                both(i, 5, g.at[zslot(-3), pl.ds(0, 2)], g.at[zslot(3), pl.ds(2, 2)], zup, zdn, zl)
            else:
                landed(i, 5)
        else:
            if s == 0:
                own = g.at[zlo, y]
                both(i, 0, own, own, zup, zdn, zl)
            elif s in (1, 2):
                landed(i, s - 1)
                both(i, s, g.at[zslot(-s), y], g.at[zslot(s), y], zup, zdn, zl)
            elif s == 3:
                landed(i, 2)
                half = g.shape[2] // 2
                both(i, 3, g.at[zslot(-3), y, pl.ds(0, half)], g.at[zslot(3), y, pl.ds(half, half)], zup, zdn, zl)
            elif s == 4:
                landed(i, 3)
                both(i, 4, g.at[:, y], g.at[:, y], yup, ydn, yl)
            elif s == 5:
                landed(i, 4)
                both(i, 5, g.at[pl.ds(0, 4), yslot(-1)], g.at[pl.ds(4, 4), yslot(1)], yup, ydn, yl)
            else:
                landed(i, 5)

    queue = sorted((LAGS[i] + s, i, s) for i in range(6) for s in range(7))
    done = [0]

    def pump(upto):
        while done[0] < len(queue) and queue[done[0]][0] <= upto:
            _, i, s = queue[done[0]]
            step(i, s)
            done[0] += 1

    rows = stream.shape[0]
    cols = stream.shape[1]
    half_rows = rows // 2
    top, low = pl.ds(0, half_rows), pl.ds(half_rows, half_rows)

    def share_start(buf):
        own = buf.at[tp]
        up = net.send(own, own, xup, "x+")
        dn = net.send(own, own, xdn, "x-")
        return [up, dn, net.send(own, own, pair, "d")]

    def share_relay(buf, got):
        pairs = [got[2]]
        left, right = xs[1] * NC + core, xs[0] * NC + core
        net.arrived(got[0])
        up = net.send(buf.at[left, top], buf.at[left, top], xup, "x+")
        pairs.append(net.send(buf.at[left], buf.at[left], pair, "d"))
        net.arrived(got[1])
        dn = net.send(buf.at[right, low], buf.at[right, low], xdn, "x-")
        pairs.append(net.send(buf.at[right], buf.at[right], pair, "d"))
        return [up, dn], pairs

    def share_finish(buf, got, pairs):
        for copy in got:
            net.arrived(copy)
        far = xfar * NC + core
        pairs.append(net.send(buf.at[far], buf.at[far], pair, "d"))
        for copy in pairs:
            net.arrived(copy)

    def norm_into(buf, gain):
        chunk = 32

        def body(r, _):
            at = pl.multiple_of(r * chunk, chunk)
            total = jnp.zeros((chunk, cols), F32)
            for b in range(NX * NC):
                v = buf[b, pl.ds(at, chunk), :].astype(F32)
                total = total + v * v
            inverse = lax.rsqrt(jnp.sum(total, axis=1, keepdims=True) * (1.0 / (cols * NX * NC)) + EPS)
            for b in range(NX * NC):
                v = buf[b, pl.ds(at, chunk), :].astype(F32)
                normed[pl.ds(at, chunk), b * cols : (b + 1) * cols] = (
                    v * inverse * gain[:, b * cols : (b + 1) * cols]
                ).astype(BF16)
            return 0

        lax.fori_loop(0, rows // chunk, body, 0)
        work(1.5)

    def weight(i):
        g = wholes[i]
        return g[...].reshape(NZ * NY * g.shape[2], g.shape[3])

    def scatter_sum(lhs, i, part, got, far, near, relay, fin, between):
        g = wholes[i]
        a = lhs[...]
        to_pair = []
        for o in (2, 1, 3, 0):
            xd = (x + o) % NX
            theirs = g[xd * NC + (1 - core)].reshape(NY * g.shape[2], g.shape[3])
            part[o] = nt(a, theirs).astype(BF16)
            to_pair.append((o, net.send(part.at[o], got.at[o], pair, "d")))
            mine = g[xd * NC + core].reshape(NY * g.shape[2], g.shape[3])
            own_sum[o] = nt(a, mine)
            work(0.7)
        pairs = dict(to_pair)
        net.arrived(pairs[2])
        far[...] = (own_sum[2] + got[2].astype(F32)).astype(BF16)
        work(0.2)
        up = net.send(far.at[top], relay.at[0], xup, "x+")
        dn = net.send(far.at[low], relay.at[1], xdn, "x-")
        net.arrived(pairs[1])
        near[0, low, :] = (own_sum[1, low, :] + got[1, low, :].astype(F32)).astype(BF16)
        up1 = net.send(near.at[0, low], fin.at[0, low], xup, "x+")
        net.arrived(pairs[3])
        near[1, top, :] = (own_sum[3, top, :] + got[3, top, :].astype(F32)).astype(BF16)
        dn1 = net.send(near.at[1, top], fin.at[1, top], xdn, "x-")
        work(0.2)
        between()
        net.arrived(up)
        near[0, top, :] = (own_sum[1, top, :] + got[1, top, :].astype(F32) + relay[0].astype(F32)).astype(BF16)
        up2 = net.send(near.at[0, top], fin.at[0, top], xup, "x+")
        net.arrived(dn)
        near[1, low, :] = (own_sum[3, low, :] + got[3, low, :].astype(F32) + relay[1].astype(F32)).astype(BF16)
        dn2 = net.send(near.at[1, low], fin.at[1, low], xdn, "x-")
        work(0.2)
        net.arrived(pairs[0])
        for copy in (up1, dn1, up2, dn2):
            net.arrived(copy)
        work(0.3)
        return own_sum[0] + got[0].astype(F32) + fin[0].astype(F32) + fin[1].astype(F32)

    got = share_start(s_all)
    pump(0)
    got, pairs = share_relay(s_all, got)
    pump(1)
    share_finish(s_all, got, pairs)
    pump(2)
    norm_into(s_all, gain_r)
    pump(6)

    rec_in = nn(normed[...], weight(0)).astype(BF16)
    pad_r[0:8, :] = jnp.zeros((8, cols), F32)
    pad_r[8:, :] = rec_in.astype(F32)
    gate_src[...] = nn(normed[...], weight(1)).astype(BF16)
    work(2.0)
    pump(7)

    heads, block = rgm.shape[0], rgm.shape[1]
    base = GATE_POWER * softplus(-rate[...])
    carry = jnp.zeros((1, cols), F32)
    piece = 64
    for r in range(rows // piece):
        lo = r * piece
        conv = rtaps[0:1, :] * pad_r[8 - 3 + lo : 8 - 3 + lo + piece, :]
        for k in range(1, 4):
            conv = conv + rtaps[k : k + 1, :] * pad_r[8 - 3 + k + lo : 8 - 3 + k + lo + piece, :]
        conv = conv.astype(BF16)
        reset, admit, jumps = [], [], []
        for h in range(heads):
            blk = conv[:, h * block : (h + 1) * block]
            reset.append(nn(blk, rgm[h]))
            admit.append(nn(blk, igm[h]))
            jumps.append(jnp.broadcast_to(spike[lo : lo + piece, h : h + 1], (piece, block)))
        reset = sigmoid(jnp.concatenate(reset, axis=1))
        admit = sigmoid(jnp.concatenate(admit, axis=1))
        log_decay = -reset * base + jnp.concatenate(jumps, axis=1)
        a = jnp.exp(log_decay)
        b = jnp.sqrt(one_minus_exp(2.0 * log_decay)) * admit * conv.astype(F32)
        row = lax.broadcasted_iota(jnp.int32, (piece, cols), 0)
        d = 1
        while d < piece:
            if d < 8:
                keep = row >= d
                pa = jnp.where(keep, pltpu.roll(a, d, 0), 1.0)
                pb = jnp.where(keep, pltpu.roll(b, d, 0), 0.0)
            else:
                pa = jnp.concatenate([jnp.ones((d, cols), F32), a[: piece - d]], axis=0)
                pb = jnp.concatenate([jnp.zeros((d, cols), F32), b[: piece - d]], axis=0)
            b = a * pb + b
            a = a * pa
            d *= 2
        states = a * carry + b
        carry = states[piece - 1 : piece, :]
        mixed[lo : lo + piece, :] = (states * gelu(gate_src[lo : lo + piece, :].astype(F32))).astype(BF16)
    work(4.0)
    pump(8)

    branch = scatter_sum(
        mixed, 2, part_a, got_a, far_a, near_a, relay_a, fin_a, lambda: pump(8)
    ).astype(BF16)
    m_all[tp] = (s_all[tp].astype(F32) + branch.astype(F32)).astype(BF16)

    got = share_start(m_all)
    pump(8)
    got, pairs = share_relay(m_all, got)
    pump(8)
    share_finish(m_all, got, pairs)
    norm_into(m_all, gain_f)
    pump(9)

    wide = g_fg.shape[3]
    for pad, i in ((pad_g, 3), (pad_v, 4)):
        pad[0:8, :] = jnp.zeros((8, wide), F32)
        for j in range(0, wide, 256):
            w = wholes[i][:, :, :, j : j + 256].reshape(NZ * NY * wholes[i].shape[2], 256)
            pad[8:, j : j + 256] = nn(normed[...], w).astype(BF16).astype(F32)
        work(2.0)
    for r in range(rows // piece):
        lo = r * piece
        gate = gtaps[0:1, :] * pad_g[6 + lo : 6 + lo + piece, :]
        value = vtaps[0:1, :] * pad_v[6 + lo : 6 + lo + piece, :]
        for k in range(1, 3):
            gate = gate + gtaps[k : k + 1, :] * pad_g[6 + k + lo : 6 + k + lo + piece, :]
            value = value + vtaps[k : k + 1, :] * pad_v[6 + k + lo : 6 + k + lo + piece, :]
        hidden[lo : lo + piece, :] = (gelu(gate) * value).astype(BF16)
    work(1.5)
    pump(99)

    branch = scatter_sum(
        hidden, 5, part_b, got_b, far_b, near_b, relay_b, fin_b, lambda: None
    ).astype(BF16)
    last = m_all[tp].astype(F32) + branch.astype(F32)
    final[...] = last
    squares = last * last
    lanes = squares[:, 0:128] + squares[:, 128:256]
    sums = jnp.sum(lanes.T, axis=0, keepdims=True)
    stats[tp] = jnp.broadcast_to(sums, (8, rows))
    sent = [net.send(stats.at[tp], stats.at[tp], device, "s") for device in others]
    for copy in sent:
        net.arrived(copy)
    total = stats[0]
    for k in range(1, NX * NC):
        total = total + stats[k]
    inverse = lax.rsqrt(total * (1.0 / (cols * NX * NC)) + EPS).T[:, 0:1]
    gain = gain_c[:, pl.ds(pl.multiple_of(tp * cols, cols), cols)]
    out[...] = (final[...] * inverse * gain).astype(BF16)
    net.drain()


def shards(
    stream, recurrence_input_weight, output_gate_weight, recurrence_gate_matrix, input_gate_matrix,
    channel_decay_rate, recurrence_taps, spike_log_decay, recurrence_output_weight, feedforward_gate_upward,
    feedforward_value_upward, feedforward_gate_taps, feedforward_value_taps, feedforward_down_weight,
    recurrence_norm_gain, feedforward_norm_gain, closing_norm_gain,
):
    rows, cols = stream.shape
    tps = NX * NC
    weights = (
        recurrence_input_weight, output_gate_weight, recurrence_output_weight.T,
        feedforward_gate_upward, feedforward_value_upward, feedforward_down_weight.T,
    )
    wide = feedforward_gate_upward.shape[1]
    hbm = pl.BlockSpec(memory_space=pltpu.MemorySpace.HBM)
    vmem = pl.BlockSpec(memory_space=pltpu.VMEM)
    scatter = [
        pltpu.VMEM((NX, rows, cols), BF16),
        pltpu.VMEM((NX, rows, cols), BF16),
        pltpu.VMEM((rows, cols), BF16),
        pltpu.VMEM((2, rows, cols), BF16),
        pltpu.VMEM((2, rows // 2, cols), BF16),
        pltpu.VMEM((2, rows, cols), BF16),
    ]
    return pl.pallas_call(
        layer_kernel,
        out_shape=jax.ShapeDtypeStruct((rows, cols), BF16),
        in_specs=[hbm] * 7 + [vmem] * 10,
        out_specs=vmem,
        scratch_shapes=[pltpu.VMEM((NZ, NY, *w.shape), BF16) for w in weights]
        + [
            pltpu.VMEM((tps, rows, cols), BF16),
            pltpu.VMEM((tps, rows, cols), BF16),
            pltpu.VMEM((rows, tps * cols), BF16),
            pltpu.VMEM((rows + 8, cols), F32),
            pltpu.VMEM((rows, cols), BF16),
            pltpu.VMEM((rows, cols), BF16),
            pltpu.VMEM((rows + 8, wide), F32),
            pltpu.VMEM((rows + 8, wide), F32),
            pltpu.VMEM((rows, wide), BF16),
            pltpu.VMEM((NX, rows, cols), F32),
        ]
        + scatter + scatter
        + [
            pltpu.VMEM((rows, cols), F32),
            pltpu.VMEM((tps, 8, rows), F32),
            pltpu.SemaphoreType.DMA((160,)),
            pltpu.SemaphoreType.DMA((160,)),
            pltpu.SemaphoreType.DMA((7,)),
        ],
        compiler_params=pltpu.CompilerParams(
            collective_id=0, has_side_effects=True, vmem_limit_bytes=60 * 1024 * 1024
        ),
        name="layer",
    )(
        stream, *weights,
        recurrence_gate_matrix, input_gate_matrix, channel_decay_rate.reshape(1, -1), recurrence_taps,
        spike_log_decay, feedforward_gate_taps, feedforward_value_taps,
        recurrence_norm_gain.reshape(1, -1), feedforward_norm_gain.reshape(1, -1), closing_norm_gain.reshape(1, -1),
    )


def solution(mesh):
    in_specs = (
        P(("rep", "fs"), "tp"), P("fs", "tp"), P("fs", "tp"), P("tp", None, None), P("tp", None, None), P("tp"),
        P(None, "tp"), P(("rep", "fs"), "tp"), P("tp", "fs"), P("fs", "tp"), P("fs", "tp"), P(None, "tp"),
        P(None, "tp"), P("tp", "fs"), P(), P(), P(),
    )
    return jax.shard_map(
        shards, mesh=mesh, in_specs=in_specs, out_specs=P(("rep", "fs"), "tp"), check_vma=False
    )
```

```python
import functools

import jax
import jax.numpy as jnp
from jax import lax
from jax.experimental import pallas as pl
from jax.experimental.pallas import tpu as pltpu
from jax.sharding import PartitionSpec as P

EPS = 1e-06
GATE_POWER = 8.0
MESH = pl.DeviceIdType.MESH
NY, NZ, NX, NC = 4, 8, 4, 2
ZRING = 16
F32, BF16 = jnp.float32, jnp.bfloat16

FIRST_Y = (True, False, True, False, False, True)
FINE = (True, True, False, False, False, False)
CHUNKS = 2
LOG = []
ORDER = (
    "w1.0", "w1.y1", "w4.0", "w1.y0", "s0", "w1.y2", "w0.00", "w2.0", "w3.0", "w5.0", "w1.1", "w1.r1", "w1.y4", "w4.1",
    "w1.r2", "w1.r0", "w1.y3", "w0.01", "w2.1", "s1", "w3.1", "w5.1", "w0.a", "w1.2", "w1.r4", "w1.y5", "w4.2", "w1.r3",
    "w1.y6", "w2.2", "s2", "w0.b", "w1.r5", "s3", "N0", "N1", "w1.3", "w4.3", "w1.r6", "w0.10", "w0.30", "w0.20",
    "w1.y7", "w3.2", "w4.4", "w0.11", "w0.31", "w0.21", "w2.3", "w0.32", "w0.22", "w0.12", "w0.02", "w2.4", "w1.r7", "w0.13",
    "w0.23", "w0.03", "w0.33", "w3.3", "w4.5", "W1", "P1", "w2.5", "w5.2", "W0", "P0", "R0", "R1", "W2",
    "R2", "w3.4", "a0m2", "a0m3", "R3", "R4", "a0f", "a0m1", "R5", "a1m2", "a0n", "a1m1", "w5.3", "a1f",
    "a0m0", "a1m0", "a0r", "W4", "a1m3", "a1n", "a1r", "a0e", "m00", "a1e", "m10", "w5.4", "w3.5", "m01",
    "m11", "m02", "m03", "M0", "m12", "u041", "u040", "m13", "w5.5", "M1", "W3", "u030", "u031", "H0",
    "H1", "u140", "H2", "u131", "u141", "W5", "b0m2", "b0m1", "b0m3", "b0f", "u130", "b0n", "H3", "H4",
    "H5", "b1m2", "b1m0", "b1m1", "b1f", "b1m3", "b0r", "b0m0", "b1n", "b1r", "b0e", "b1e", "F0", "F1",
)


class Net:
    def __init__(self, ssem, rsem):
        self.ssem, self.rsem = ssem, rsem
        self.copies = {}
        self.taken = set()

    def send(self, key, src, dst, device, link):
        i = len(self.copies)
        copy = pltpu.make_async_remote_copy(
            src_ref=src, dst_ref=dst, send_sem=self.ssem.at[i], recv_sem=self.rsem.at[i],
            device_id=device, device_id_type=MESH,
        )
        copy.start()
        n = 1
        for s in src.shape:
            n *= s
        LOG.append(("start", link, n * src.dtype.itemsize, key))
        self.copies[key] = copy

    def take(self, *keys):
        for key in keys:
            if key not in self.taken:
                self.taken.add(key)
                LOG.append(("wait", key))
                with scope("wait_" + str(key)):
                    self.copies[key].wait_recv()

    def drain(self):
        for copy in self.copies.values():
            copy.wait_send()


def scope(name):
    return jax.named_scope(name)


def work(us):
    LOG.append(("work", us))


def sigmoid(v):
    return 1.0 / (1.0 + jnp.exp(-v))


def gelu(v):
    return 0.5 * v * (1.0 + jnp.tanh(0.7978845608028654 * (v + 0.044715 * (v * v * v))))


def softplus(v):
    t = jnp.exp(-jnp.abs(v))
    u = 1.0 + t
    small = u == 1.0
    log1p = jnp.where(small, t, jnp.log(u) * (t / jnp.where(small, 1.0, u - 1.0)))
    return jnp.maximum(v, 0.0) + log1p


def one_minus_exp(v):
    term = 1.0 + v * (1.0 / 9.0)
    for k in (8, 7, 6, 5, 4, 3, 2):
        term = 1.0 + v * (1.0 / k) * term
    return jnp.where(v > -0.5, -v * term, 1.0 - jnp.exp(v))


def nn(a, b):
    return lax.dot_general(a, b, (((1,), (0,)), ((), ())), preferred_element_type=F32)


def nt(a, b):
    return lax.dot_general(a, b, (((1,), (1,)), ((), ())), preferred_element_type=F32)


def layer_kernel(
    stream, w_in, w_gate, w_out, w_fg, w_fv, w_down,
    rgm, igm, rate, rtaps, spike, gtaps, vtaps, gain_r, gain_f, gain_c,
    out,
    g_in, g_gate, g_out, g_fg, g_fv, g_down,
    s_all, m_all, normed, pad_r, gate_src, mixed, pad_g, pad_v, hidden, carry,
    own_a, part_a, got_a, far_a, near_a, relay_a, fin_a,
    own_b, part_b, got_b, far_b, near_b, relay_b, fin_b,
    final, stats, ssem, rsem, lsem,
):
    rep, fs, tp = lax.axis_index("rep"), lax.axis_index("fs"), lax.axis_index("tp")
    zlo, y = fs // NY, fs % NY
    x, core = tp // NC, tp % NC
    z = rep * NZ + zlo
    zs = [(z + k) % ZRING for k in (1, ZRING - 1)]
    ys = [(y + k) % NY for k in (1, NY - 1)]
    xs = [(x + k) % NX for k in (1, NX - 1)]

    def at_z(zz):
        return {"rep": zz // NZ, "fs": (zz % NZ) * NY + y, "tp": tp}

    def at_y(yy):
        return {"rep": rep, "fs": zlo * NY + yy, "tp": tp}

    def at_x(xx, cc):
        return {"rep": rep, "fs": fs, "tp": xx * NC + cc}

    zup, zdn = at_z(zs[0]), at_z(zs[1])
    yup, ydn = at_y(ys[0]), at_y(ys[1])
    xup, xdn = at_x(xs[0], core), at_x(xs[1], core)
    pair = at_x(x, 1 - core)
    xfar = (x + 2) % NX

    shards = (w_in, w_gate, w_out, w_fg, w_fv, w_down)
    wholes = (g_in, g_gate, g_out, g_fg, g_fv, g_down)
    loads = [pltpu.make_async_copy(stream, s_all.at[tp], lsem.at[6])]
    for i in range(6):
        loads.append(pltpu.make_async_copy(shards[i], wholes[i].at[zlo, y], lsem.at[i]))
    for copy in loads:
        copy.start()

    others = [at_x(xx, cc) for xx in (xs[0], xs[1], xfar) for cc in (core, 1 - core)] + [pair]
    with scope("barrier"):
        barrier = pltpu.get_barrier_semaphore()
        friends = [zup, zdn, yup, ydn] + others
        for friend in friends:
            pl.semaphore_signal(barrier, inc=1, device_id=friend, device_id_type=MESH)
        pl.semaphore_wait(barrier, len(friends))
    with scope("loads"):
        for copy in loads:
            copy.wait()

    net = Net(ssem, rsem)
    items = {}

    def item(name, deps, *args):
        def add(fn):
            items[name] = (tuple(deps), functools.partial(fn, *args))
            return fn
        return add

    def zslot(k):
        return (zlo + k + NZ) % NZ

    def yslot(k):
        return (y + k + NY) % NY

    def both(key, up_src, dn_src, line):
        up, dn = (zup, zdn) if line == "z" else (yup, ydn)
        net.send(key + "+", up_src, up_src, up, line + "+")
        net.send(key + "-", dn_src, dn_src, dn, line + "-")

    def landed(key):
        net.take(key + "+", key + "-")

    def coarse(i, g):
        n = f"w{i}."
        half = g.shape[2] // 2
        steps = []
        if FIRST_Y[i]:
            steps = [
                lambda: both(n + "0", g.at[zlo, y], g.at[zlo, y], "y"),
                lambda: both(n + "1", g.at[zlo, yslot(-1), pl.ds(0, half)], g.at[zlo, yslot(1), pl.ds(half, half)], "y"),
                lambda: both(n + "2", g.at[zlo], g.at[zlo], "z"),
                lambda: both(n + "3", g.at[zslot(-1)], g.at[zslot(1)], "z"),
                lambda: both(n + "4", g.at[zslot(-2)], g.at[zslot(2)], "z"),
                lambda: both(n + "5", g.at[zslot(-3), pl.ds(0, 2)], g.at[zslot(3), pl.ds(2, 2)], "z"),
            ]
        else:
            steps = [
                lambda: both(n + "0", g.at[zlo, y], g.at[zlo, y], "z"),
                lambda: both(n + "1", g.at[zslot(-1), y], g.at[zslot(1), y], "z"),
                lambda: both(n + "2", g.at[zslot(-2), y], g.at[zslot(2), y], "z"),
                lambda: both(n + "3", g.at[zslot(-3), y, pl.ds(0, half)], g.at[zslot(3), y, pl.ds(half, half)], "z"),
                lambda: both(n + "4", g.at[:, y], g.at[:, y], "y"),
                lambda: both(n + "5", g.at[pl.ds(0, 4), yslot(-1)], g.at[pl.ds(4, 4), yslot(1)], "y"),
            ]

        def run(s):
            if s > 0:
                landed(n + str(s - 1))
            steps[s]()

        for s in range(6):
            item(n + str(s), [n + str(s - 1)] if s else [], s)(run)
        item(f"W{i}", [n + "5"])(lambda: landed(n + "5"))

    def fine_y(i, g):
        n = f"w{i}."
        half = g.shape[2] // 2
        item(n + "a", [])(lambda: both(n + "a", g.at[zlo, y], g.at[zlo, y], "y"))

        def relay():
            landed(n + "a")
            both(n + "b", g.at[zlo, yslot(-1), pl.ds(0, half)], g.at[zlo, yslot(1), pl.ds(half, half)], "y")

        item(n + "b", [n + "a"])(relay)
        before = ([], [n + "a"], [n + "a"], [n + "b"])

        def hop(j, o, k):
            if k == 0:
                if j == 1:
                    net.take(n + "a+")
                elif j == 2:
                    net.take(n + "a-")
                elif j == 3:
                    landed(n + "b")
            else:
                landed(f"{n}{j}{k - 1}")
            yy = yslot(o)
            if k < 3:
                both(f"{n}{j}{k}", g.at[zslot(-k), yy], g.at[zslot(k), yy], "z")
            else:
                both(f"{n}{j}{k}", g.at[zslot(-3), yy, pl.ds(0, half)], g.at[zslot(3), yy, pl.ds(half, half)], "z")

        for j, o in enumerate((0, -1, 1, 2)):
            for k in range(4):
                item(f"{n}{j}{k}", [f"{n}{j}{k - 1}"] if k else before[j], j, o, k)(hop)

        def end():
            for j in range(4):
                landed(f"{n}{j}3")

        item(f"W{i}", [f"{n}{j}3" for j in range(4)] + [n + "b"])(end)

    def fine_z(i, g):
        n = f"w{i}."
        half = g.shape[2] // 2

        def hop(k):
            if k:
                landed(f"{n}{k - 1}")
            if k < 3:
                both(f"{n}{k}", g.at[zslot(-k), y], g.at[zslot(k), y], "z")
            else:
                both(f"{n}{k}", g.at[zslot(-3), y, pl.ds(0, half)], g.at[zslot(3), y, pl.ds(half, half)], "z")

        for k in range(4):
            item(f"{n}{k}", [f"{n}{k - 1}"] if k else [], k)(hop)

        def side(m, o):
            if o == 4:
                landed(f"{n}3")
            elif o < 0:
                net.take(f"{n}{-o - 1}+")
            elif o > 0:
                net.take(f"{n}{o - 1}-")
            both(f"{n}y{m}", g.at[zslot(o), y], g.at[zslot(o), y], "y")

        def relay(m, o):
            landed(f"{n}y{m}")
            both(f"{n}r{m}", g.at[zslot(o), yslot(-1), pl.ds(0, half)], g.at[zslot(o), yslot(1), pl.ds(half, half)], "y")

        ms = (0, -1, 1, -2, 2, -3, 3, 4)
        for m, o in enumerate(ms):
            item(f"{n}y{m}", [f"{n}{abs(o) - 1}"] if o else [], m, o)(side)
            item(f"{n}r{m}", [f"{n}y{m}"], m, o)(relay)

        def end():
            for m in range(8):
                landed(f"{n}r{m}")

        item(f"W{i}", [f"{n}r{m}" for m in range(8)])(end)

    for i in range(6):
        if FINE[i]:
            (fine_y if FIRST_Y[i] else fine_z)(i, wholes[i])
        else:
            coarse(i, wholes[i])

    rows, cols = stream.shape
    span = rows // CHUNKS
    half_rows = span // 2

    def share(n, buf, lo, size, deps):
        whole, top, low = pl.ds(lo, size), pl.ds(lo, size // 2), pl.ds(lo + size // 2, size // 2)
        left, right, far = xs[1] * NC + core, xs[0] * NC + core, xfar * NC + core

        def start():
            own = buf.at[tp, whole]
            net.send(n + "0+", own, own, xup, "x+")
            net.send(n + "0-", own, own, xdn, "x-")
            net.send(n + "p0", own, own, pair, "d")

        def relay():
            net.take(n + "0+")
            net.send(n + "1+", buf.at[left, top], buf.at[left, top], xup, "x+")
            net.take(n + "0-")
            net.send(n + "1-", buf.at[right, low], buf.at[right, low], xdn, "x-")
            net.send(n + "p1", buf.at[left, whole], buf.at[left, whole], pair, "d")
            net.send(n + "p2", buf.at[right, whole], buf.at[right, whole], pair, "d")

        def last():
            net.take(n + "1+", n + "1-")
            net.send(n + "p3", buf.at[far, whole], buf.at[far, whole], pair, "d")

        item(n + "0", deps)(start)
        item(n + "1", [n + "0"])(relay)
        item(n + "2", [n + "1"])(last)
        item(n + "3", [n + "2"])(lambda: net.take(n + "p0", n + "p1", n + "p2", n + "p3"))

    chunk = 32

    def norm_rows(buf, gain, lo, size):
        def body(r, _):
            at = pl.multiple_of(lo + r * chunk, chunk)
            total = jnp.zeros((chunk, cols), F32)
            for b in range(NX * NC):
                v = buf[b, pl.ds(at, chunk), :].astype(F32)
                total = total + v * v
            inverse = lax.rsqrt(jnp.sum(total, axis=1, keepdims=True) * (1.0 / (cols * NX * NC)) + EPS)
            for b in range(NX * NC):
                v = buf[b, pl.ds(at, chunk), :].astype(F32)
                normed[pl.ds(at, chunk), b * cols : (b + 1) * cols] = (
                    v * inverse * gain[:, b * cols : (b + 1) * cols]
                ).astype(BF16)
            return 0

        lax.fori_loop(0, size // chunk, body, 0)
        work(1.5 * size / 384)

    def scatter(n, t, lhs, i, own, part, got, far, near, relay, fin, deps, finish):
        g = wholes[i]
        lo = t * span
        top, low = slice(0, half_rows), slice(half_rows, span)

        def mm(o):
            a = lhs[lo : lo + span, :]
            xd = (x + o) % NX
            theirs = g[xd * NC + (1 - core)].reshape(NY * g.shape[2], g.shape[3])
            part[t, o] = nt(a, theirs).astype(BF16)
            net.send(f"{n}d{o}", part.at[t, o], got.at[t, o], pair, "d")
            mine = g[xd * NC + core].reshape(NY * g.shape[2], g.shape[3])
            own[t, o] = nt(a, mine)
            work(0.4)

        def out_far():
            net.take(n + "d2")
            far[t] = (own[t, 2] + got[t, 2].astype(F32)).astype(BF16)
            work(0.1)
            net.send(n + "f+", far.at[t, pl.ds(0, half_rows)], relay.at[t, 0], xup, "x+")
            net.send(n + "f-", far.at[t, pl.ds(half_rows, half_rows)], relay.at[t, 1], xdn, "x-")

        def out_near():
            net.take(n + "d1", n + "d3")
            near[t, 0, low, :] = (own[t, 1, low, :] + got[t, 1, low, :].astype(F32)).astype(BF16)
            near[t, 1, top, :] = (own[t, 3, top, :] + got[t, 3, top, :].astype(F32)).astype(BF16)
            work(0.1)
            at = pl.ds(half_rows, half_rows)
            net.send(n + "n+", near.at[t, 0, at], fin.at[t, 0, at], xup, "x+")
            at = pl.ds(0, half_rows)
            net.send(n + "n-", near.at[t, 1, at], fin.at[t, 1, at], xdn, "x-")

        def out_relay():
            net.take(n + "f+", n + "f-")
            near[t, 0, top, :] = (own[t, 1, top, :] + got[t, 1, top, :].astype(F32) + relay[t, 0].astype(F32)).astype(BF16)
            near[t, 1, low, :] = (own[t, 3, low, :] + got[t, 3, low, :].astype(F32) + relay[t, 1].astype(F32)).astype(BF16)
            work(0.1)
            at = pl.ds(0, half_rows)
            net.send(n + "r+", near.at[t, 0, at], fin.at[t, 0, at], xup, "x+")
            at = pl.ds(half_rows, half_rows)
            net.send(n + "r-", near.at[t, 1, at], fin.at[t, 1, at], xdn, "x-")

        def end():
            net.take(n + "d0", n + "n+", n + "n-", n + "r+", n + "r-")
            finish(own[t, 0] + got[t, 0].astype(F32) + fin[t, 0].astype(F32) + fin[t, 1].astype(F32))

        for o in (2, 1, 3, 0):
            item(f"{n}m{o}", deps, o)(mm)
        item(n + "f", [n + "m2"])(out_far)
        item(n + "n", [n + "m1", n + "m3"])(out_near)
        item(n + "r", [n + "f", n + "n"])(out_relay)
        item(n + "e", [n + "r", n + "m0"])(end)

    share("s", s_all, 0, rows, [])
    for t in range(2):
        item(f"N{t}", ["s3"], s_all, gain_r, t * rows // 2, rows // 2)(norm_rows)

    def weight(i, j=0, n=0):
        g = wholes[i]
        return g[:, :, :, j : j + (n or g.shape[3])].reshape(NZ * NY * g.shape[2], n or g.shape[3])

    def project_in():
        rec_in = nn(normed[...], weight(0)).astype(BF16)
        pad_r[0:8, :] = jnp.zeros((8, cols), F32)
        pad_r[8:, :] = rec_in.astype(F32)
        work(1.0)

    def project_gate():
        gate_src[...] = nn(normed[...], weight(1)).astype(BF16)
        work(1.0)

    item("P0", ["N0", "N1", "W0"])(project_in)
    item("P1", ["N0", "N1", "W1"])(project_gate)

    heads, block = rgm.shape[0], rgm.shape[1]
    piece = 64

    def recur(r):
        base = GATE_POWER * softplus(-rate[...])
        lo = r * piece
        conv = rtaps[0:1, :] * pad_r[8 - 3 + lo : 8 - 3 + lo + piece, :]
        for k in range(1, 4):
            conv = conv + rtaps[k : k + 1, :] * pad_r[8 - 3 + k + lo : 8 - 3 + k + lo + piece, :]
        conv = conv.astype(BF16)
        reset, admit, jumps = [], [], []
        for h in range(heads):
            blk = conv[:, h * block : (h + 1) * block]
            reset.append(nn(blk, rgm[h]))
            admit.append(nn(blk, igm[h]))
            jumps.append(jnp.broadcast_to(spike[lo : lo + piece, h : h + 1], (piece, block)))
        reset = sigmoid(jnp.concatenate(reset, axis=1))
        admit = sigmoid(jnp.concatenate(admit, axis=1))
        log_decay = -reset * base + jnp.concatenate(jumps, axis=1)
        a = jnp.exp(log_decay)
        b = jnp.sqrt(one_minus_exp(2.0 * log_decay)) * admit * conv.astype(F32)
        row = lax.broadcasted_iota(jnp.int32, (piece, cols), 0)
        d = 1
        while d < piece:
            if d < 8:
                keep = row >= d
                pa = jnp.where(keep, pltpu.roll(a, d, 0), 1.0)
                pb = jnp.where(keep, pltpu.roll(b, d, 0), 0.0)
            else:
                pa = jnp.concatenate([jnp.ones((d, cols), F32), a[: piece - d]], axis=0)
                pb = jnp.concatenate([jnp.zeros((d, cols), F32), b[: piece - d]], axis=0)
            b = a * pb + b
            a = a * pa
            d *= 2
        states = b if r == 0 else a * carry[0:1, :] + b
        carry[0:1, :] = states[piece - 1 : piece, :]
        mixed[lo : lo + piece, :] = (states * gelu(gate_src[lo : lo + piece, :].astype(F32))).astype(BF16)
        work(0.7)

    per = span // piece
    for r in range(rows // piece):
        item(f"R{r}", ["P0", "P1"] + ([f"R{r - 1}"] if r else []), r)(recur)

    def to_middle(t, total):
        at = slice(t * span, (t + 1) * span)
        m_all[tp, at, :] = (s_all[tp, at, :].astype(F32) + total.astype(BF16).astype(F32)).astype(BF16)
        work(0.15)

    for t in range(CHUNKS):
        scatter(
            f"a{t}", t, mixed, 2, own_a, part_a, got_a, far_a, near_a, relay_a, fin_a,
            ["W2"] + [f"R{t * per + q}" for q in range(per)], functools.partial(to_middle, t),
        )
        share(f"m{t}", m_all, t * span, span, [f"a{t}e"])
        item(f"M{t}", [f"m{t}3", "P0", "P1"], m_all, gain_f, t * span, span)(norm_rows)

    wide = g_fg.shape[3]

    def up(t, i, pad, j):
        at = slice(t * span, (t + 1) * span)
        if t == 0:
            pad[0:8, j : j + 256] = jnp.zeros((8, 256), F32)
        pad[8 + t * span : 8 + (t + 1) * span, j : j + 256] = nn(normed[at, :], weight(i, j, 256)).astype(BF16).astype(F32)
        work(0.6)

    def mix(r):
        lo = r * piece
        gate = gtaps[0:1, :] * pad_g[6 + lo : 6 + lo + piece, :]
        value = vtaps[0:1, :] * pad_v[6 + lo : 6 + lo + piece, :]
        for k in range(1, 3):
            gate = gate + gtaps[k : k + 1, :] * pad_g[6 + k + lo : 6 + k + lo + piece, :]
            value = value + vtaps[k : k + 1, :] * pad_v[6 + k + lo : 6 + k + lo + piece, :]
        hidden[lo : lo + piece, :] = (gelu(gate) * value).astype(BF16)
        work(0.3)

    def to_final(t, total):
        at = slice(t * span, (t + 1) * span)
        last = m_all[tp, at, :].astype(F32) + total.astype(BF16).astype(F32)
        final[at, :] = last
        squares = last * last
        lanes = squares[:, 0:128] + squares[:, 128:256]
        sums = jnp.sum(lanes.T, axis=0, keepdims=True)
        stats[t, tp] = jnp.broadcast_to(sums, (8, span))
        work(0.5)
        for k, device in enumerate(others):
            net.send(f"q{t}{k}", stats.at[t, tp], stats.at[t, tp], device, "s")

    def finish(t):
        for k in range(len(others)):
            net.take(f"q{t}{k}")
        at = slice(t * span, (t + 1) * span)
        total = stats[t, 0]
        for k in range(1, NX * NC):
            total = total + stats[t, k]
        inverse = lax.rsqrt(total * (1.0 / (cols * NX * NC)) + EPS).T[:, 0:1]
        gain = gain_c[:, pl.ds(pl.multiple_of(tp * cols, cols), cols)]
        out[at, :] = (final[at, :] * inverse * gain).astype(BF16)
        work(0.4)

    for t in range(CHUNKS):
        ups = []
        for i, pad in ((3, pad_g), (4, pad_v)):
            for j in range(0, wide, 256):
                ups.append(f"u{t}{i}{j // 256}")
                item(ups[-1], [f"M{t}", f"W{i}"], t, i, pad, j)(up)
        for q in range(per):
            r = t * per + q
            item(f"H{r}", ups + ([f"H{r - 1}"] if r else []), r)(mix)
        scatter(
            f"b{t}", t, hidden, 5, own_b, part_b, got_b, far_b, near_b, relay_b, fin_b,
            ["W5"] + [f"H{t * per + q}" for q in range(per)], functools.partial(to_final, t),
        )
        item(f"F{t}", [f"b{t}e"])(functools.partial(finish, t))

    emitted = set()

    def emit(name):
        if name in emitted:
            return
        deps, fn = items[name]
        for dep in deps:
            emit(dep)
        LOG.append(("item", name, deps))
        with scope(name):
            fn()
        emitted.add(name)

    for name in ORDER:
        emit(name)
    for name in items:
        emit(name)
    LOG.append(("item", "drain", tuple(items)))
    with scope("drain"):
        net.drain()


def shards(
    stream, recurrence_input_weight, output_gate_weight, recurrence_gate_matrix, input_gate_matrix,
    channel_decay_rate, recurrence_taps, spike_log_decay, recurrence_output_weight, feedforward_gate_upward,
    feedforward_value_upward, feedforward_gate_taps, feedforward_value_taps, feedforward_down_weight,
    recurrence_norm_gain, feedforward_norm_gain, closing_norm_gain,
):
    rows, cols = stream.shape
    tps = NX * NC
    weights = (
        recurrence_input_weight, output_gate_weight, recurrence_output_weight.T,
        feedforward_gate_upward, feedforward_value_upward, feedforward_down_weight.T,
    )
    wide = feedforward_gate_upward.shape[1]
    hbm = pl.BlockSpec(memory_space=pltpu.MemorySpace.HBM)
    vmem = pl.BlockSpec(memory_space=pltpu.VMEM)
    span = rows // CHUNKS
    scatter = [
        pltpu.VMEM((CHUNKS, NX, span, cols), F32),
        pltpu.VMEM((CHUNKS, NX, span, cols), BF16),
        pltpu.VMEM((CHUNKS, NX, span, cols), BF16),
        pltpu.VMEM((CHUNKS, span, cols), BF16),
        pltpu.VMEM((CHUNKS, 2, span, cols), BF16),
        pltpu.VMEM((CHUNKS, 2, span // 2, cols), BF16),
        pltpu.VMEM((CHUNKS, 2, span, cols), BF16),
    ]
    return pl.pallas_call(
        layer_kernel,
        out_shape=jax.ShapeDtypeStruct((rows, cols), BF16),
        in_specs=[hbm] * 7 + [vmem] * 10,
        out_specs=vmem,
        scratch_shapes=[pltpu.VMEM((NZ, NY, *w.shape), BF16) for w in weights]
        + [
            pltpu.VMEM((tps, rows, cols), BF16),
            pltpu.VMEM((tps, rows, cols), BF16),
            pltpu.VMEM((rows, tps * cols), BF16),
            pltpu.VMEM((rows + 8, cols), F32),
            pltpu.VMEM((rows, cols), BF16),
            pltpu.VMEM((rows, cols), BF16),
            pltpu.VMEM((rows + 8, wide), F32),
            pltpu.VMEM((rows + 8, wide), F32),
            pltpu.VMEM((rows, wide), BF16),
            pltpu.VMEM((8, cols), F32),
        ]
        + scatter + scatter
        + [
            pltpu.VMEM((rows, cols), F32),
            pltpu.VMEM((CHUNKS, tps, 8, span), F32),
            pltpu.SemaphoreType.DMA((288,)),
            pltpu.SemaphoreType.DMA((288,)),
            pltpu.SemaphoreType.DMA((7,)),
        ],
        compiler_params=pltpu.CompilerParams(
            collective_id=0, has_side_effects=True, vmem_limit_bytes=60 * 1024 * 1024
        ),
        name="layer",
    )(
        stream, *weights,
        recurrence_gate_matrix, input_gate_matrix, channel_decay_rate.reshape(1, -1), recurrence_taps,
        spike_log_decay, feedforward_gate_taps, feedforward_value_taps,
        recurrence_norm_gain.reshape(1, -1), feedforward_norm_gain.reshape(1, -1), closing_norm_gain.reshape(1, -1),
    )


def solution(mesh):
    in_specs = (
        P(("rep", "fs"), "tp"), P("fs", "tp"), P("fs", "tp"), P("tp", None, None), P("tp", None, None), P("tp"),
        P(None, "tp"), P(("rep", "fs"), "tp"), P("tp", "fs"), P("fs", "tp"), P("fs", "tp"), P(None, "tp"),
        P(None, "tp"), P("tp", "fs"), P(), P(), P(),
    )
    return jax.shard_map(
        shards, mesh=mesh, in_specs=in_specs, out_specs=P(("rep", "fs"), "tp"), check_vma=False
    )
```

```python
import functools

import jax
import jax.numpy as jnp
from jax import lax
from jax.experimental import pallas as pl
from jax.experimental.pallas import tpu as pltpu
from jax.sharding import PartitionSpec as P

EPS = 1e-06
GATE_POWER = 8.0
MESH = pl.DeviceIdType.MESH
NY, NZ, NX, NC = 4, 8, 4, 2
ZRING = 16
F32, BF16 = jnp.float32, jnp.bfloat16

FIRST_Y = (True, False, True, False, False, True)
FINE = (True, True, True, True, True, True)
CHUNKS = 2
SEMS = 145
LOG = []
ORDER = (
    42, 40, 0, 19, 120, 128, 129, 2, 23, 59, 63, 80, 101, 46, 1, 41, 20, 24, 27, 10, 65, 6,
    121, 3, 86, 14, 47, 31, 21, 29, 54, 28, 7, 66, 11, 25, 122, 15, 64, 4, 32, 33, 123, 124,
    22, 35, 50, 125, 8, 30, 84, 12, 16, 26, 43, 102, 55, 37, 51, 36, 34, 9, 67, 13, 5, 17,
    48, 85, 44, 87, 56, 38, 88, 52, 81, 18, 126, 68, 49, 45, 39, 127, 53, 57, 130, 60, 89, 131,
    132, 82, 92, 133, 134, 135, 115, 90, 58, 149, 151, 150, 71, 61, 152, 153, 136, 69, 138, 154, 83, 139,
    94, 107, 137, 140, 103, 96, 155, 141, 62, 72, 111, 73, 142, 108, 70, 156, 157, 75, 116, 77, 104, 143,
    144, 74, 112, 95, 97, 158, 109, 76, 98, 117, 145, 78, 105, 93, 159, 91, 113, 160, 161, 146, 110, 99,
    118, 79, 178, 179, 106, 147, 148, 162, 114, 163, 100, 181, 164, 180, 165, 166, 167, 168, 119, 182, 183, 184,
    169, 171, 173, 170, 185, 172, 174, 186, 175, 187, 176, 188, 177, 189,
)


class Net:
    def __init__(self, ssem, rsem):
        self.ssem, self.rsem = ssem, rsem
        self.arrivals, self.departures = {}, {}
        self.taken = set()

    def send(self, key, leave, src, dst, device, link):
        copy = pltpu.make_async_remote_copy(
            src_ref=src, dst_ref=dst,
            send_sem=self.ssem.at[self.departures.setdefault(leave, len(self.departures))],
            recv_sem=self.rsem.at[self.arrivals.setdefault(key, len(self.arrivals))],
            device_id=device, device_id_type=MESH,
        )
        copy.start()
        n = 1
        for size in src.shape:
            n *= size
        LOG.append(("start", link, n * src.dtype.itemsize, key))

    def take(self, key, ref):
        LOG.append(("wait", key))
        if key not in self.taken:
            self.taken.add(key)
            with scope("wait_" + key):
                pltpu.make_async_copy(ref, ref, self.rsem.at[self.arrivals[key]]).wait()

    def left(self, leave, ref):
        pltpu.make_async_copy(ref, ref, self.ssem.at[self.departures.pop(leave)]).wait()


def scope(name):
    return jax.named_scope(name)


def work(us):
    LOG.append(("work", us))


def sigmoid(v):
    return 1.0 / (1.0 + jnp.exp(-v))


def gelu(v):
    return 0.5 * v * (1.0 + jnp.tanh(0.7978845608028654 * (v + 0.044715 * (v * v * v))))


def softplus(v):
    t = jnp.exp(-jnp.abs(v))
    u = 1.0 + t
    small = u == 1.0
    log1p = jnp.where(small, t, jnp.log(u) * (t / jnp.where(small, 1.0, u - 1.0)))
    return jnp.maximum(v, 0.0) + log1p


def one_minus_exp(v):
    term = 1.0 + v * (1.0 / 9.0)
    for k in (8, 7, 6, 5, 4, 3, 2):
        term = 1.0 + v * (1.0 / k) * term
    return jnp.where(v > -0.5, -v * term, 1.0 - jnp.exp(v))


def nn(a, b):
    return lax.dot_general(a, b, (((1,), (0,)), ((), ())), preferred_element_type=F32)


def nt(a, b):
    return lax.dot_general(a, b, (((1,), (1,)), ((), ())), preferred_element_type=F32)


def layer_kernel(
    stream, w_in, w_gate, w_out, w_fg, w_fv, w_down,
    rgm_h, igm_h, rate_h, rtaps_h, spike_h, gtaps_h, vtaps_h, gain_r_h, gain_f_h, gain_c_h,
    out,
    g_in, g_gate, g_out, g_fg, g_fv, g_down,
    s_all, m_all, normed, pad_r, gate_src, mixed, pad_g, pad_v, hidden, carry,
    own_a, part_a, got_a, far_a, near_a, relay_a, fin_a,
    own_b, part_b, got_b, far_b, near_b, relay_b, fin_b,
    final, stats, jumpt,
    rgm, igm, rate, rtaps, spike, gtaps, vtaps, gain_r, gain_f, gain_c,
    ssem, rsem, lsem,
):
    rep, fs, tp = lax.axis_index("rep"), lax.axis_index("fs"), lax.axis_index("tp")
    zlo, y = fs // NY, fs % NY
    x, core = tp // NC, tp % NC
    z = rep * NZ + zlo
    zs = [(z + k) % ZRING for k in (1, ZRING - 1)]
    ys = [(y + k) % NY for k in (1, NY - 1)]
    xs = [(x + k) % NX for k in (1, NX - 1)]

    def at_z(zz):
        return {"rep": zz // NZ, "fs": (zz % NZ) * NY + y, "tp": tp}

    def at_y(yy):
        return {"rep": rep, "fs": zlo * NY + yy, "tp": tp}

    def at_x(xx, cc):
        return {"rep": rep, "fs": fs, "tp": xx * NC + cc}

    zup, zdn = at_z(zs[0]), at_z(zs[1])
    yup, ydn = at_y(ys[0]), at_y(ys[1])
    xup, xdn = at_x(xs[0], core), at_x(xs[1], core)
    pair = at_x(x, 1 - core)
    xfar = (x + 2) % NX

    shards = (w_in, w_gate, w_out, w_fg, w_fv, w_down)
    wholes = (g_in, g_gate, g_out, g_fg, g_fv, g_down)
    loads = [pltpu.make_async_copy(stream, s_all.at[tp], lsem.at[6])]
    for i in range(6):
        loads.append(pltpu.make_async_copy(shards[i], wholes[i].at[zlo, y], lsem.at[i]))
    far_small = (rgm_h, igm_h, rate_h, rtaps_h, spike_h, gtaps_h, vtaps_h, gain_r_h, gain_f_h, gain_c_h)
    small = (rgm, igm, rate, rtaps, spike, gtaps, vtaps, gain_r, gain_f, gain_c)
    for i in range(len(small)):
        loads.append(pltpu.make_async_copy(far_small[i], small[i], lsem.at[7 + i]))
    for copy in loads:
        copy.start()

    others = [at_x(xx, cc) for xx in (xs[0], xs[1], xfar) for cc in (core, 1 - core)] + [pair]
    with scope("barrier"):
        barrier = pltpu.get_barrier_semaphore()
        friends = [zup, zdn, yup, ydn] + others
        for friend in friends:
            pl.semaphore_signal(barrier, inc=1, device_id=friend, device_id_type=MESH)
        pl.semaphore_wait(barrier, len(friends))
    with scope("loads"):
        for copy in loads[:7]:
            copy.wait()

    net = Net(ssem, rsem)
    items, ends = {}, []

    def item(name, deps, *args):
        def add(fn):
            items[name] = (tuple(deps), functools.partial(fn, *args))
            return fn
        return add

    def zslot(k):
        return (zlo + k + NZ) % NZ

    def yslot(k):
        return (y + k + NY) % NY

    def both(i, key, up_src, dn_src, line):
        up, dn = (zup, zdn) if line == "z" else (yup, ydn)
        net.send(key, f"{i}{line}", up_src, up_src, up, line + "+")
        net.send(key, f"{i}{line}", dn_src, dn_src, dn, line + "-")

    def coarse(i, g):
        n = f"w{i}."
        half = g.shape[2] // 2
        if FIRST_Y[i]:
            steps = [
                ("y", g.at[zlo, y], g.at[zlo, y], g.at[0, pl.ds(0, 2)]),
                ("y", g.at[zlo, yslot(-1), pl.ds(0, half)], g.at[zlo, yslot(1), pl.ds(half, half)], g.at[0, 0]),
                ("z", g.at[zlo], g.at[zlo], g.at[pl.ds(0, 2)]),
                ("z", g.at[zslot(-1)], g.at[zslot(1)], g.at[pl.ds(0, 2)]),
                ("z", g.at[zslot(-2)], g.at[zslot(2)], g.at[pl.ds(0, 2)]),
                ("z", g.at[zslot(-3), pl.ds(0, 2)], g.at[zslot(3), pl.ds(2, 2)], g.at[0]),
            ]
        else:
            steps = [
                ("z", g.at[zlo, y], g.at[zlo, y], g.at[0, pl.ds(0, 2)]),
                ("z", g.at[zslot(-1), y], g.at[zslot(1), y], g.at[0, pl.ds(0, 2)]),
                ("z", g.at[zslot(-2), y], g.at[zslot(2), y], g.at[0, pl.ds(0, 2)]),
                ("z", g.at[zslot(-3), y, pl.ds(0, half)], g.at[zslot(3), y, pl.ds(half, half)], g.at[0, 0]),
                ("y", g.at[:, y], g.at[:, y], g.at[pl.ds(0, 4)]),
                ("y", g.at[pl.ds(0, 4), yslot(-1)], g.at[pl.ds(4, 4), yslot(1)], g.at[pl.ds(0, 2)]),
            ]

        def run(s):
            if s > 0:
                net.take(n + str(s - 1), steps[s - 1][3])
            if s < 6:
                both(i, n + str(s), steps[s][1], steps[s][2], steps[s][0])

        for s in range(6):
            item(n + str(s), [n + str(s - 1)] if s else [], s)(run)
        item(f"W{i}", [n + "5"], 6)(run)

    def fine_y(i, g):
        n = f"w{i}."
        half = g.shape[2] // 2
        two, one = g.at[0, pl.ds(0, 2)], g.at[0, 0]
        item(n + "a", [])(lambda: both(i, n + "a", g.at[zlo, y], g.at[zlo, y], "y"))

        def relay():
            net.take(n + "a", two)
            both(i, n + "b", g.at[zlo, yslot(-1), pl.ds(0, half)], g.at[zlo, yslot(1), pl.ds(half, half)], "y")

        item(n + "b", [n + "a"])(relay)
        before = ([], [n + "a"], [n + "a"], [n + "b"])

        def hop(j, o, k):
            if k == 0:
                if j in (1, 2):
                    net.take(n + "a", two)
                elif j == 3:
                    net.take(n + "b", one)
            else:
                net.take(f"{n}{j}{k - 1}", two)
            yy = yslot(o)
            if k < 3:
                both(i, f"{n}{j}{k}", g.at[zslot(-k), yy], g.at[zslot(k), yy], "z")
            else:
                both(i, f"{n}{j}{k}", g.at[zslot(-3), yy, pl.ds(0, half)], g.at[zslot(3), yy, pl.ds(half, half)], "z")

        for j, o in enumerate((0, -1, 1, 2)):
            for k in range(4):
                item(f"{n}{j}{k}", [f"{n}{j}{k - 1}"] if k else before[j], j, o, k)(hop)

        def end():
            for j in range(4):
                net.take(f"{n}{j}3", one)

        item(f"W{i}", [f"{n}{j}3" for j in range(4)] + [n + "b"])(end)

    def fine_z(i, g):
        n = f"w{i}."
        half = g.shape[2] // 2
        two, one = g.at[0, pl.ds(0, 2)], g.at[0, 0]

        def hop(k):
            if k:
                net.take(f"{n}{k - 1}", two)
            if k < 3:
                both(i, f"{n}{k}", g.at[zslot(-k), y], g.at[zslot(k), y], "z")
            else:
                both(i, f"{n}{k}", g.at[zslot(-3), y, pl.ds(0, half)], g.at[zslot(3), y, pl.ds(half, half)], "z")

        for k in range(4):
            item(f"{n}{k}", [f"{n}{k - 1}"] if k else [], k)(hop)

        def side(m, o):
            if o == 4:
                net.take(f"{n}3", one)
            elif o:
                net.take(f"{n}{abs(o) - 1}", two)
            both(i, f"{n}y{m}", g.at[zslot(o), y], g.at[zslot(o), y], "y")

        def relay(m, o):
            net.take(f"{n}y{m}", two)
            both(i, f"{n}r{m}", g.at[zslot(o), yslot(-1), pl.ds(0, half)], g.at[zslot(o), yslot(1), pl.ds(half, half)], "y")

        ms = (0, -1, 1, -2, 2, -3, 3, 4)
        for m, o in enumerate(ms):
            item(f"{n}y{m}", [f"{n}{abs(o) - 1}"] if o else [], m, o)(side)
            item(f"{n}r{m}", [f"{n}y{m}"], m, o)(relay)

        def end():
            for m in range(8):
                net.take(f"{n}r{m}", one)

        item(f"W{i}", [f"{n}r{m}" for m in range(8)])(end)

    for i, g in enumerate(wholes):
        if FIRST_Y[i]:
            ends += [(f"{i}y", g.at[0, pl.ds(0, 3)]), (f"{i}z", g.at[pl.ds(0, 7)])]
        else:
            ends += [(f"{i}z", g.at[pl.ds(0, 7), 0]), (f"{i}y", g.at[pl.ds(0, 6)])]
        if FINE[i]:
            (fine_y if FIRST_Y[i] else fine_z)(i, wholes[i])
        else:
            coarse(i, wholes[i])

    rows, cols = stream.shape
    span = rows // CHUNKS
    half_rows = span // 2

    def share(n, buf, lo, size, deps):
        whole, top, low = pl.ds(lo, size), pl.ds(lo, size // 2), pl.ds(lo + size // 2, size // 2)
        left, right, far = xs[1] * NC + core, xs[0] * NC + core, xfar * NC + core

        def start():
            own = buf.at[tp, whole]
            net.send(n + "0", n + "x", own, own, xup, "x+")
            net.send(n + "0", n + "x", own, own, xdn, "x-")
            net.send(n + "p", n + "p", own, own, pair, "d")

        def relay():
            net.take(n + "0", buf.at[pl.ds(0, 2), whole])
            net.send(n + "1", n + "x", buf.at[left, top], buf.at[left, top], xup, "x+")
            net.send(n + "1", n + "x", buf.at[right, low], buf.at[right, low], xdn, "x-")
            net.send(n + "p", n + "p", buf.at[left, whole], buf.at[left, whole], pair, "d")
            net.send(n + "p", n + "p", buf.at[right, whole], buf.at[right, whole], pair, "d")

        def last():
            net.take(n + "1", buf.at[0, whole])
            net.send(n + "p", n + "p", buf.at[far, whole], buf.at[far, whole], pair, "d")

        def settle():
            net.take(n + "p", buf.at[pl.ds(0, 4), whole])

        ends.append((n + "x", buf.at[pl.ds(0, 3), whole]))
        ends.append((n + "p", buf.at[pl.ds(0, 4), whole]))
        item(n + "0", deps)(start)
        item(n + "1", [n + "0"])(relay)
        item(n + "2", [n + "1"])(last)
        item(n + "3", [n + "2"])(settle)

    chunk = 32

    def norm_rows(buf, gain, lo, size):
        def body(r, _):
            at = pl.multiple_of(lo + r * chunk, chunk)
            total = jnp.zeros((chunk, cols), F32)
            for b in range(NX * NC):
                v = buf[b, pl.ds(at, chunk), :].astype(F32)
                total = total + v * v
            inverse = lax.rsqrt(jnp.sum(total, axis=1, keepdims=True) * (1.0 / (cols * NX * NC)) + EPS)
            for b in range(NX * NC):
                v = buf[b, pl.ds(at, chunk), :].astype(F32)
                normed[pl.ds(at, chunk), b * cols : (b + 1) * cols] = (
                    v * inverse * gain[:, b * cols : (b + 1) * cols]
                ).astype(BF16)
            return 0

        lax.fori_loop(0, size // chunk, body, 0)
        work(1.5 * size / 384)

    def scatter(n, t, lhs, i, own, part, got, far, near, relay, fin, deps, finish, joint=False):
        g = wholes[i]
        lo = t * span
        top, low = slice(0, half_rows), slice(half_rows, span)

        def mm(o):
            a = lhs[lo : lo + span, :]
            xd = (x + o) % NX
            theirs = g[xd * NC + (1 - core)].reshape(NY * g.shape[2], g.shape[3])
            part[t, o] = nt(a, theirs).astype(BF16)
            net.send(f"{n}d{o % 2 or o}", n + "d", part.at[t, o], got.at[t, o], pair, "d")
            mine = g[xd * NC + core].reshape(NY * g.shape[2], g.shape[3])
            own[t, o] = nt(a, mine)
            work(0.4)

        def out_far():
            net.take(n + "d2", got.at[t, 2])
            far[t] = (own[t, 2] + got[t, 2].astype(F32)).astype(BF16)
            work(0.1)
            net.send(n + "f", n + "f", far.at[t, pl.ds(0, half_rows)], relay.at[t, 0], xup, "x+")
            net.send(n + "f", n + "f", far.at[t, pl.ds(half_rows, half_rows)], relay.at[t, 1], xdn, "x-")

        def out_near():
            net.take(n + "d1", got.at[t, pl.ds(0, 2)])
            near[t, 0, low, :] = (own[t, 1, low, :] + got[t, 1, low, :].astype(F32)).astype(BF16)
            near[t, 1, top, :] = (own[t, 3, top, :] + got[t, 3, top, :].astype(F32)).astype(BF16)
            work(0.1)
            at = pl.ds(half_rows, half_rows)
            net.send(n + "e", n + "e", near.at[t, 0, at], fin.at[t, 0, at], xup, "x+")
            at = pl.ds(0, half_rows)
            net.send(n + "e", n + "e", near.at[t, 1, at], fin.at[t, 1, at], xdn, "x-")

        def out_relay():
            net.take(n + "f", relay.at[t])
            near[t, 0, top, :] = (own[t, 1, top, :] + got[t, 1, top, :].astype(F32) + relay[t, 0].astype(F32)).astype(BF16)
            near[t, 1, low, :] = (own[t, 3, low, :] + got[t, 3, low, :].astype(F32) + relay[t, 1].astype(F32)).astype(BF16)
            work(0.1)
            at = pl.ds(0, half_rows)
            net.send(n + "e", n + "e", near.at[t, 0, at], fin.at[t, 0, at], xup, "x+")
            at = pl.ds(half_rows, half_rows)
            net.send(n + "e", n + "e", near.at[t, 1, at], fin.at[t, 1, at], xdn, "x-")

        def end():
            net.take(n + "d0", got.at[t, 0])
            net.take(n + "e", fin.at[t])
            finish(own[t, 0] + got[t, 0].astype(F32) + fin[t, 0].astype(F32) + fin[t, 1].astype(F32))

        ends.append((n + "d", part.at[t]))
        ends.append((n + "f", far.at[t]))
        ends.append((n + "e", near.at[t]))
        def mm_joint(o):
            a = lhs[...]
            xd = (x + o) % NX
            theirs = g[xd * NC + (1 - core)].reshape(NY * g.shape[2], g.shape[3])
            terms = nt(a, theirs).astype(BF16)
            for c in range(CHUNKS):
                part[c, o] = terms[c * span : (c + 1) * span]
                net.send(f"{n[0]}{c}d{o % 2 or o}", f"{n[0]}{c}d", part.at[c, o], got.at[c, o], pair, "d")
            mine = g[xd * NC + core].reshape(NY * g.shape[2], g.shape[3])
            terms = nt(a, mine)
            for c in range(CHUNKS):
                own[c, o] = terms[c * span : (c + 1) * span]
            work(0.9)

        m = n[0] + "m" if joint else n + "m"
        if not joint or t == 0:
            for o in (2, 1, 3, 0):
                item(f"{m}{o}", deps, o)(mm_joint if joint else mm)
        item(n + "f", [m + "2"])(out_far)
        item(n + "n", [m + "1", m + "3"])(out_near)
        item(n + "r", [n + "f", n + "n"])(out_relay)
        item(n + "e", [n + "r", m + "0"])(end)

    share("s", s_all, 0, rows, [])
    for t in range(2):
        item(f"N{t}", ["s3", "L"], s_all, gain_r, t * rows // 2, rows // 2)(norm_rows)

    def weight(i, j=0, n=0):
        g = wholes[i]
        return g[:, :, :, j : j + (n or g.shape[3])].reshape(NZ * NY * g.shape[2], n or g.shape[3])

    def project_in():
        rec_in = nn(normed[...], weight(0)).astype(BF16)
        pad_r[0:8, :] = jnp.zeros((8, cols), F32)
        pad_r[8:, :] = rec_in.astype(F32)
        work(1.0)

    def project_gate():
        gate_src[...] = nn(normed[...], weight(1)).astype(BF16)
        work(1.0)

    item("P0", ["N0", "N1", "W0"])(project_in)
    item("P1", ["N0", "N1", "W1"])(project_gate)

    heads, block = rgm.shape[0], rgm.shape[1]

    def jump():
        wide_rows = jnp.concatenate([spike[...], jnp.zeros((8 - heads, rows), F32)], axis=0)
        jumpt[...] = wide_rows.T

    def settled():
        for copy in loads[7:]:
            copy.wait()

    item("L", [])(settled)
    item("J", ["L"])(jump)
    piece = 64

    def recur(r):
        base = GATE_POWER * softplus(-rate[...])
        lo = r * piece
        conv = rtaps[0:1, :] * pad_r[8 - 3 + lo : 8 - 3 + lo + piece, :]
        for k in range(1, 4):
            conv = conv + rtaps[k : k + 1, :] * pad_r[8 - 3 + k + lo : 8 - 3 + k + lo + piece, :]
        conv = conv.astype(BF16)
        reset, admit, jumps = [], [], []
        for h in range(heads):
            blk = conv[:, h * block : (h + 1) * block]
            reset.append(nn(blk, rgm[h]))
            admit.append(nn(blk, igm[h]))
            jumps.append(jnp.broadcast_to(jumpt[lo : lo + piece, h : h + 1], (piece, block)))
        reset = sigmoid(jnp.concatenate(reset, axis=1))
        admit = sigmoid(jnp.concatenate(admit, axis=1))
        log_decay = -reset * base + jnp.concatenate(jumps, axis=1)
        a = jnp.exp(log_decay)
        b = jnp.sqrt(one_minus_exp(2.0 * log_decay)) * admit * conv.astype(F32)
        row = lax.broadcasted_iota(jnp.int32, (piece, cols), 0)
        d = 1
        while d < piece:
            if d < 8:
                keep = row >= d
                pa = jnp.where(keep, pltpu.roll(a, d, 0), 1.0)
                pb = jnp.where(keep, pltpu.roll(b, d, 0), 0.0)
            else:
                pa = jnp.concatenate([jnp.ones((d, cols), F32), a[: piece - d]], axis=0)
                pb = jnp.concatenate([jnp.zeros((d, cols), F32), b[: piece - d]], axis=0)
            b = a * pb + b
            a = a * pa
            d *= 2
        states = b if r == 0 else a * carry[0:1, :] + b
        carry[0:1, :] = states[piece - 1 : piece, :]
        mixed[lo : lo + piece, :] = (states * gelu(gate_src[lo : lo + piece, :].astype(F32))).astype(BF16)
        work(0.7)

    per = span // piece
    for r in range(rows // piece):
        item(f"R{r}", ["P0", "P1", "J"] + ([f"R{r - 1}"] if r else []), r)(recur)

    def to_middle(t, total):
        at = slice(t * span, (t + 1) * span)
        m_all[tp, at, :] = (s_all[tp, at, :].astype(F32) + total.astype(BF16).astype(F32)).astype(BF16)
        work(0.15)

    for t in range(CHUNKS):
        scatter(
            f"a{t}", t, mixed, 2, own_a, part_a, got_a, far_a, near_a, relay_a, fin_a,
            ["W2"] + [f"R{t * per + q}" for q in range(per)], functools.partial(to_middle, t),
        )
        share(f"m{t}", m_all, t * span, span, [f"a{t}e"])
        item(f"M{t}", [f"m{t}3", "P0", "P1"], m_all, gain_f, t * span, span)(norm_rows)

    wide = g_fg.shape[3]

    def up(t, i, pad, j):
        at = slice(t * span, (t + 1) * span)
        if t == 0:
            pad[0:8, j : j + 256] = jnp.zeros((8, 256), F32)
        pad[8 + t * span : 8 + (t + 1) * span, j : j + 256] = nn(normed[at, :], weight(i, j, 256)).astype(BF16).astype(F32)
        work(0.6)

    def mix(r):
        lo = r * piece
        gate = gtaps[0:1, :] * pad_g[6 + lo : 6 + lo + piece, :]
        value = vtaps[0:1, :] * pad_v[6 + lo : 6 + lo + piece, :]
        for k in range(1, 3):
            gate = gate + gtaps[k : k + 1, :] * pad_g[6 + k + lo : 6 + k + lo + piece, :]
            value = value + vtaps[k : k + 1, :] * pad_v[6 + k + lo : 6 + k + lo + piece, :]
        hidden[lo : lo + piece, :] = (gelu(gate) * value).astype(BF16)
        work(0.3)

    def to_final(t, total):
        at = slice(t * span, (t + 1) * span)
        last = m_all[tp, at, :].astype(F32) + total.astype(BF16).astype(F32)
        final[at, :] = last
        squares = last * last
        lanes = squares[:, 0:128] + squares[:, 128:256]
        sums = jnp.sum(lanes.T, axis=0, keepdims=True)
        stats[t, tp] = jnp.broadcast_to(sums, (8, span))
        work(0.5)
        for device in others:
            net.send(f"q{t}", f"q{t}", stats.at[t, tp], stats.at[t, tp], device, "s")

    def finish(t):
        net.take(f"q{t}", stats.at[t, pl.ds(0, 7)])
        at = slice(t * span, (t + 1) * span)
        total = stats[t, 0]
        for k in range(1, NX * NC):
            total = total + stats[t, k]
        inverse = lax.rsqrt(total * (1.0 / (cols * NX * NC)) + EPS).T[:, 0:1]
        gain = gain_c[:, pl.ds(pl.multiple_of(tp * cols, cols), cols)]
        out[at, :] = (final[at, :] * inverse * gain).astype(BF16)
        work(0.4)

    for t in range(CHUNKS):
        ups = []
        for i, pad in ((3, pad_g), (4, pad_v)):
            for j in range(0, wide, 256):
                ups.append(f"u{t}{i}{j // 256}")
                item(ups[-1], [f"M{t}", f"W{i}"], t, i, pad, j)(up)
        for q in range(per):
            r = t * per + q
            item(f"H{r}", ups + ([f"H{r - 1}"] if r else []), r)(mix)
        scatter(
            f"b{t}", t, hidden, 5, own_b, part_b, got_b, far_b, near_b, relay_b, fin_b,
            ["W5"] + [f"H{q}" for q in range(rows // piece)], functools.partial(to_final, t), True,
        )
        ends.append((f"q{t}", stats.at[t, pl.ds(0, 7)]))
        item(f"F{t}", [f"b{t}e"])(functools.partial(finish, t))

    emitted = set()

    def emit(name):
        if name in emitted:
            return
        deps, fn = items[name]
        for dep in deps:
            emit(dep)
        LOG.append(("item", name, deps))
        with scope(name):
            fn()
        emitted.add(name)

    names = tuple(items)
    for k in ORDER:
        emit(names[k])
    for name in names:
        emit(name)
    LOG.append(("names", names))
    LOG.append(("item", "drain", tuple(items)))
    with scope("drain"):
        for leave, ref in ends:
            net.left(leave, ref)
    assert not net.departures and set(net.arrivals) == net.taken, "unbalanced"
    LOG.append(("counts", len(net.arrivals), len(ends)))


def shards(
    stream, recurrence_input_weight, output_gate_weight, recurrence_gate_matrix, input_gate_matrix,
    channel_decay_rate, recurrence_taps, spike_log_decay, recurrence_output_weight, feedforward_gate_upward,
    feedforward_value_upward, feedforward_gate_taps, feedforward_value_taps, feedforward_down_weight,
    recurrence_norm_gain, feedforward_norm_gain, closing_norm_gain,
):
    rows, cols = stream.shape
    tps = NX * NC
    weights = (
        recurrence_input_weight, output_gate_weight, recurrence_output_weight.T,
        feedforward_gate_upward, feedforward_value_upward, feedforward_down_weight.T,
    )
    wide = feedforward_gate_upward.shape[1]
    hbm = pl.BlockSpec(memory_space=pltpu.MemorySpace.HBM)
    vmem = pl.BlockSpec(memory_space=pltpu.VMEM)
    small = (
        recurrence_gate_matrix, input_gate_matrix, channel_decay_rate.reshape(1, -1), recurrence_taps,
        spike_log_decay.T, feedforward_gate_taps, feedforward_value_taps,
        recurrence_norm_gain.reshape(1, -1), feedforward_norm_gain.reshape(1, -1), closing_norm_gain.reshape(1, -1),
    )
    span = rows // CHUNKS
    scatter = [
        pltpu.VMEM((CHUNKS, NX, span, cols), F32),
        pltpu.VMEM((CHUNKS, NX, span, cols), BF16),
        pltpu.VMEM((CHUNKS, NX, span, cols), BF16),
        pltpu.VMEM((CHUNKS, span, cols), BF16),
        pltpu.VMEM((CHUNKS, 2, span, cols), BF16),
        pltpu.VMEM((CHUNKS, 2, span // 2, cols), BF16),
        pltpu.VMEM((CHUNKS, 2, span, cols), BF16),
    ]
    return pl.pallas_call(
        layer_kernel,
        out_shape=jax.ShapeDtypeStruct((rows, cols), BF16),
        in_specs=[hbm] * 17,
        out_specs=vmem,
        scratch_shapes=[pltpu.VMEM((NZ, NY, *w.shape), BF16) for w in weights]
        + [
            pltpu.VMEM((tps, rows, cols), BF16),
            pltpu.VMEM((tps, rows, cols), BF16),
            pltpu.VMEM((rows, tps * cols), BF16),
            pltpu.VMEM((rows + 8, cols), F32),
            pltpu.VMEM((rows, cols), BF16),
            pltpu.VMEM((rows, cols), BF16),
            pltpu.VMEM((rows + 8, wide), F32),
            pltpu.VMEM((rows + 8, wide), F32),
            pltpu.VMEM((rows, wide), BF16),
            pltpu.VMEM((8, cols), F32),
        ]
        + scatter + scatter
        + [
            pltpu.VMEM((rows, cols), F32),
            pltpu.VMEM((CHUNKS, tps, 8, span), F32),
            pltpu.VMEM((rows, 8), F32),
        ]
        + [pltpu.VMEM(v.shape, v.dtype) for v in small]
        + [
            pltpu.SemaphoreType.DMA((32,)),
            pltpu.SemaphoreType.DMA((SEMS,)),
            pltpu.SemaphoreType.DMA((17,)),
        ],
        compiler_params=pltpu.CompilerParams(
            collective_id=0, has_side_effects=True, vmem_limit_bytes=60 * 1024 * 1024
        ),
        name="layer",
    )(
        stream, *weights, *small,
    )


def solution(mesh):
    in_specs = (
        P(("rep", "fs"), "tp"), P("fs", "tp"), P("fs", "tp"), P("tp", None, None), P("tp", None, None), P("tp"),
        P(None, "tp"), P(("rep", "fs"), "tp"), P("tp", "fs"), P("fs", "tp"), P("fs", "tp"), P(None, "tp"),
        P(None, "tp"), P("tp", "fs"), P(), P(), P(),
    )
    return jax.shard_map(
        shards, mesh=mesh, in_specs=in_specs, out_specs=P(("rep", "fs"), "tp"), check_vma=False
    )
```

```python
import functools

import jax
import jax.numpy as jnp
from jax import lax
from jax.experimental import pallas as pl
from jax.experimental.pallas import tpu as pltpu
from jax.sharding import PartitionSpec as P

EPS = 1e-06
GATE_POWER = 8.0
MESH = pl.DeviceIdType.MESH
NY, NZ, NX, NC = 4, 8, 4, 2
ZRING = 16
F32, BF16 = jnp.float32, jnp.bfloat16

FIRST_Y = (True, False, True, False, False, True)
FINE = (True, True, True, True, True, True)
CHUNKS = 2
SEMS = 145
LOG = []
ORDER = (
    42, 0, 101, 120, 19, 2, 59, 84, 10, 1, 23, 40, 20, 25, 3, 80, 11, 14, 65, 29, 41, 27,
    6, 26, 46, 121, 86, 50, 21, 24, 15, 30, 102, 12, 43, 31, 7, 22, 122, 4, 28, 33, 63, 54,
    51, 16, 35, 128, 123, 32, 129, 47, 8, 37, 67, 34, 55, 13, 52, 36, 124, 17, 5, 38, 9, 44,
    48, 56, 81, 66, 88, 125, 39, 127, 53, 18, 87, 45, 126, 49, 130, 57, 64, 85, 60, 68, 131, 132,
    133, 92, 82, 111, 134, 135, 58, 136, 90, 138, 89, 69, 61, 71, 149, 137, 94, 115, 83, 96, 140, 103,
    150, 151, 112, 141, 139, 142, 62, 72, 73, 152, 153, 116, 107, 75, 143, 144, 77, 104, 98, 154, 117, 70,
    74, 108, 93, 76, 113, 145, 155, 78, 99, 105, 91, 95, 97, 109, 146, 156, 157, 114, 118, 79, 147, 148,
    159, 106, 158, 110, 100, 160, 161, 162, 163, 164, 174, 175, 176, 119, 165, 167, 169, 166, 177, 170, 168, 178,
    171, 179, 172, 180, 173, 181,
)


class Net:
    def __init__(self, ssem, rsem):
        self.ssem, self.rsem = ssem, rsem
        self.arrivals, self.departures = {}, {}
        self.taken = set()

    def send(self, key, leave, src, dst, device, link):
        copy = pltpu.make_async_remote_copy(
            src_ref=src, dst_ref=dst,
            send_sem=self.ssem.at[self.departures.setdefault(leave, len(self.departures))],
            recv_sem=self.rsem.at[self.arrivals.setdefault(key, len(self.arrivals))],
            device_id=device, device_id_type=MESH,
        )
        copy.start()
        n = 1
        for size in src.shape:
            n *= size
        LOG.append(("start", link, n * src.dtype.itemsize, key))

    def take(self, key, ref):
        LOG.append(("wait", key))
        if key not in self.taken:
            self.taken.add(key)
            with scope("wait_" + key):
                pltpu.make_async_copy(ref, ref, self.rsem.at[self.arrivals[key]]).wait()

    def left(self, leave, ref):
        pltpu.make_async_copy(ref, ref, self.ssem.at[self.departures.pop(leave)]).wait()


def scope(name):
    return jax.named_scope(name)


def work(us):
    LOG.append(("work", us))


def sigmoid(v):
    return 1.0 / (1.0 + jnp.exp(-v))


def gelu(v):
    return 0.5 * v * (1.0 + jnp.tanh(0.7978845608028654 * (v + 0.044715 * (v * v * v))))


def softplus(v):
    t = jnp.exp(-jnp.abs(v))
    u = 1.0 + t
    small = u == 1.0
    log1p = jnp.where(small, t, jnp.log(u) * (t / jnp.where(small, 1.0, u - 1.0)))
    return jnp.maximum(v, 0.0) + log1p


def one_minus_exp(v):
    term = 1.0 + v * (1.0 / 9.0)
    for k in (8, 7, 6, 5, 4, 3, 2):
        term = 1.0 + v * (1.0 / k) * term
    return jnp.where(v > -0.5, -v * term, 1.0 - jnp.exp(v))


def nn(a, b):
    return lax.dot_general(a, b, (((1,), (0,)), ((), ())), preferred_element_type=F32)


def nt(a, b):
    return lax.dot_general(a, b, (((1,), (1,)), ((), ())), preferred_element_type=F32)


def layer_kernel(
    stream, w_in, w_gate, w_out, w_fg, w_fv, w_down,
    rgm_h, igm_h, rate_h, rtaps_h, spike_h, gtaps_h, vtaps_h, gain_r_h, gain_f_h, gain_c_h,
    out,
    g_in, g_gate, g_out, g_fg, g_fv, g_down,
    s_all, m_all, normed, pad_r, gate_src, mixed, pad_g, pad_v, hidden, carry,
    own_a, part_a, got_a, far_a, near_a, relay_a, fin_a,
    own_b, part_b, got_b, far_b, near_b, relay_b, fin_b,
    final, stats, jumpt,
    rgm, igm, rate, rtaps, spike, gtaps, vtaps, gain_r, gain_f, gain_c,
    ssem, rsem, lsem,
):
    rep, fs, tp = lax.axis_index("rep"), lax.axis_index("fs"), lax.axis_index("tp")
    zlo, y = fs // NY, fs % NY
    x, core = tp // NC, tp % NC
    z = rep * NZ + zlo
    zs = [(z + k) % ZRING for k in (1, ZRING - 1)]
    ys = [(y + k) % NY for k in (1, NY - 1)]
    xs = [(x + k) % NX for k in (1, NX - 1)]

    def at_z(zz):
        return {"rep": zz // NZ, "fs": (zz % NZ) * NY + y, "tp": tp}

    def at_y(yy):
        return {"rep": rep, "fs": zlo * NY + yy, "tp": tp}

    def at_x(xx, cc):
        return {"rep": rep, "fs": fs, "tp": xx * NC + cc}

    zup, zdn = at_z(zs[0]), at_z(zs[1])
    yup, ydn = at_y(ys[0]), at_y(ys[1])
    xup, xdn = at_x(xs[0], core), at_x(xs[1], core)
    pair = at_x(x, 1 - core)
    xfar = (x + 2) % NX

    shards = (w_in, w_gate, w_out, w_fg, w_fv, w_down)
    wholes = (g_in, g_gate, g_out, g_fg, g_fv, g_down)
    loads = [pltpu.make_async_copy(stream, s_all.at[tp], lsem.at[6])]
    for i in range(6):
        loads.append(pltpu.make_async_copy(shards[i], wholes[i].at[zlo, y], lsem.at[i]))
    far_small = (rgm_h, igm_h, rate_h, rtaps_h, spike_h, gtaps_h, vtaps_h, gain_r_h, gain_f_h, gain_c_h)
    small = (rgm, igm, rate, rtaps, spike, gtaps, vtaps, gain_r, gain_f, gain_c)
    for i in range(len(small)):
        loads.append(pltpu.make_async_copy(far_small[i], small[i], lsem.at[7 + i]))
    for copy in loads:
        copy.start()

    others = [at_x(xx, cc) for xx in (xs[0], xs[1], xfar) for cc in (core, 1 - core)] + [pair]
    with scope("barrier"):
        barrier = pltpu.get_barrier_semaphore()
        friends = [zup, zdn, yup, ydn] + others
        for friend in friends:
            pl.semaphore_signal(barrier, inc=1, device_id=friend, device_id_type=MESH)
        pl.semaphore_wait(barrier, len(friends))
    with scope("loads"):
        for copy in loads[:7]:
            copy.wait()

    net = Net(ssem, rsem)
    items, ends = {}, []

    def item(name, deps, *args):
        def add(fn):
            items[name] = (tuple(deps), functools.partial(fn, *args))
            return fn
        return add

    def zslot(k):
        return (zlo + k + NZ) % NZ

    def yslot(k):
        return (y + k + NY) % NY

    def both(i, key, up_src, dn_src, line):
        up, dn = (zup, zdn) if line == "z" else (yup, ydn)
        net.send(key, f"{i}{line}", up_src, up_src, up, line + "+")
        net.send(key, f"{i}{line}", dn_src, dn_src, dn, line + "-")

    def coarse(i, g):
        n = f"w{i}."
        half = g.shape[2] // 2
        if FIRST_Y[i]:
            steps = [
                ("y", g.at[zlo, y], g.at[zlo, y], g.at[0, pl.ds(0, 2)]),
                ("y", g.at[zlo, yslot(-1), pl.ds(0, half)], g.at[zlo, yslot(1), pl.ds(half, half)], g.at[0, 0]),
                ("z", g.at[zlo], g.at[zlo], g.at[pl.ds(0, 2)]),
                ("z", g.at[zslot(-1)], g.at[zslot(1)], g.at[pl.ds(0, 2)]),
                ("z", g.at[zslot(-2)], g.at[zslot(2)], g.at[pl.ds(0, 2)]),
                ("z", g.at[zslot(-3), pl.ds(0, 2)], g.at[zslot(3), pl.ds(2, 2)], g.at[0]),
            ]
        else:
            steps = [
                ("z", g.at[zlo, y], g.at[zlo, y], g.at[0, pl.ds(0, 2)]),
                ("z", g.at[zslot(-1), y], g.at[zslot(1), y], g.at[0, pl.ds(0, 2)]),
                ("z", g.at[zslot(-2), y], g.at[zslot(2), y], g.at[0, pl.ds(0, 2)]),
                ("z", g.at[zslot(-3), y, pl.ds(0, half)], g.at[zslot(3), y, pl.ds(half, half)], g.at[0, 0]),
                ("y", g.at[:, y], g.at[:, y], g.at[pl.ds(0, 4)]),
                ("y", g.at[pl.ds(0, 4), yslot(-1)], g.at[pl.ds(4, 4), yslot(1)], g.at[pl.ds(0, 2)]),
            ]

        def run(s):
            if s > 0:
                net.take(n + str(s - 1), steps[s - 1][3])
            if s < 6:
                both(i, n + str(s), steps[s][1], steps[s][2], steps[s][0])

        for s in range(6):
            item(n + str(s), [n + str(s - 1)] if s else [], s)(run)
        item(f"W{i}", [n + "5"], 6)(run)

    def fine_y(i, g):
        n = f"w{i}."
        half = g.shape[2] // 2
        two, one = g.at[0, pl.ds(0, 2)], g.at[0, 0]
        item(n + "a", [])(lambda: both(i, n + "a", g.at[zlo, y], g.at[zlo, y], "y"))

        def relay():
            net.take(n + "a", two)
            both(i, n + "b", g.at[zlo, yslot(-1), pl.ds(0, half)], g.at[zlo, yslot(1), pl.ds(half, half)], "y")

        item(n + "b", [n + "a"])(relay)
        before = ([], [n + "a"], [n + "a"], [n + "b"])

        def hop(j, o, k):
            if k == 0:
                if j in (1, 2):
                    net.take(n + "a", two)
                elif j == 3:
                    net.take(n + "b", one)
            else:
                net.take(f"{n}{j}{k - 1}", two)
            yy = yslot(o)
            if k < 3:
                both(i, f"{n}{j}{k}", g.at[zslot(-k), yy], g.at[zslot(k), yy], "z")
            else:
                both(i, f"{n}{j}{k}", g.at[zslot(-3), yy, pl.ds(0, half)], g.at[zslot(3), yy, pl.ds(half, half)], "z")

        for j, o in enumerate((0, -1, 1, 2)):
            for k in range(4):
                item(f"{n}{j}{k}", [f"{n}{j}{k - 1}"] if k else before[j], j, o, k)(hop)

        def end():
            for j in range(4):
                net.take(f"{n}{j}3", one)

        item(f"W{i}", [f"{n}{j}3" for j in range(4)] + [n + "b"])(end)

    def fine_z(i, g):
        n = f"w{i}."
        half = g.shape[2] // 2
        two, one = g.at[0, pl.ds(0, 2)], g.at[0, 0]

        def hop(k):
            if k:
                net.take(f"{n}{k - 1}", two)
            if k < 3:
                both(i, f"{n}{k}", g.at[zslot(-k), y], g.at[zslot(k), y], "z")
            else:
                both(i, f"{n}{k}", g.at[zslot(-3), y, pl.ds(0, half)], g.at[zslot(3), y, pl.ds(half, half)], "z")

        for k in range(4):
            item(f"{n}{k}", [f"{n}{k - 1}"] if k else [], k)(hop)

        def side(m, o):
            if o == 4:
                net.take(f"{n}3", one)
            elif o:
                net.take(f"{n}{abs(o) - 1}", two)
            both(i, f"{n}y{m}", g.at[zslot(o), y], g.at[zslot(o), y], "y")

        def relay(m, o):
            net.take(f"{n}y{m}", two)
            both(i, f"{n}r{m}", g.at[zslot(o), yslot(-1), pl.ds(0, half)], g.at[zslot(o), yslot(1), pl.ds(half, half)], "y")

        ms = (0, -1, 1, -2, 2, -3, 3, 4)
        for m, o in enumerate(ms):
            item(f"{n}y{m}", [f"{n}{abs(o) - 1}"] if o else [], m, o)(side)
            item(f"{n}r{m}", [f"{n}y{m}"], m, o)(relay)

        def end():
            for m in range(8):
                net.take(f"{n}r{m}", one)

        item(f"W{i}", [f"{n}r{m}" for m in range(8)])(end)

    for i, g in enumerate(wholes):
        if FIRST_Y[i]:
            ends += [(f"{i}y", g.at[0, pl.ds(0, 3)]), (f"{i}z", g.at[pl.ds(0, 7)])]
        else:
            ends += [(f"{i}z", g.at[pl.ds(0, 7), 0]), (f"{i}y", g.at[pl.ds(0, 6)])]
        if FINE[i]:
            (fine_y if FIRST_Y[i] else fine_z)(i, wholes[i])
        else:
            coarse(i, wholes[i])

    rows, cols = stream.shape
    span = rows // CHUNKS
    half_rows = span // 2

    def share(n, buf, lo, size, deps):
        whole, top, low = pl.ds(lo, size), pl.ds(lo, size // 2), pl.ds(lo + size // 2, size // 2)
        left, right, far = xs[1] * NC + core, xs[0] * NC + core, xfar * NC + core

        def start():
            own = buf.at[tp, whole]
            net.send(n + "0", n + "x", own, own, xup, "x+")
            net.send(n + "0", n + "x", own, own, xdn, "x-")
            net.send(n + "p", n + "p", own, own, pair, "d")

        def relay():
            net.take(n + "0", buf.at[pl.ds(0, 2), whole])
            net.send(n + "1", n + "x", buf.at[left, top], buf.at[left, top], xup, "x+")
            net.send(n + "1", n + "x", buf.at[right, low], buf.at[right, low], xdn, "x-")
            net.send(n + "p", n + "p", buf.at[left, whole], buf.at[left, whole], pair, "d")
            net.send(n + "p", n + "p", buf.at[right, whole], buf.at[right, whole], pair, "d")

        def last():
            net.take(n + "1", buf.at[0, whole])
            net.send(n + "p", n + "p", buf.at[far, whole], buf.at[far, whole], pair, "d")

        def settle():
            net.take(n + "p", buf.at[pl.ds(0, 4), whole])

        ends.append((n + "x", buf.at[pl.ds(0, 3), whole]))
        ends.append((n + "p", buf.at[pl.ds(0, 4), whole]))
        item(n + "0", deps)(start)
        item(n + "1", [n + "0"])(relay)
        item(n + "2", [n + "1"])(last)
        item(n + "3", [n + "2"])(settle)

    chunk = 32

    def norm_rows(buf, gain, lo, size):
        def body(r, _):
            at = pl.multiple_of(lo + r * chunk, chunk)
            total = jnp.zeros((chunk, cols), F32)
            for b in range(NX * NC):
                v = buf[b, pl.ds(at, chunk), :].astype(F32)
                total = total + v * v
            inverse = lax.rsqrt(jnp.sum(total, axis=1, keepdims=True) * (1.0 / (cols * NX * NC)) + EPS)
            for b in range(NX * NC):
                v = buf[b, pl.ds(at, chunk), :].astype(F32)
                normed[pl.ds(at, chunk), b * cols : (b + 1) * cols] = (
                    v * inverse * gain[:, b * cols : (b + 1) * cols]
                ).astype(BF16)
            return 0

        lax.fori_loop(0, size // chunk, body, 0)
        work(1.5 * size / 384)

    def scatter(n, t, lhs, i, own, part, got, far, near, relay, fin, deps, finish, joint=False):
        g = wholes[i]
        lo = t * span
        top, low = slice(0, half_rows), slice(half_rows, span)

        def mm(o):
            a = lhs[lo : lo + span, :]
            xd = (x + o) % NX
            theirs = g[xd * NC + (1 - core)].reshape(NY * g.shape[2], g.shape[3])
            part[t, o] = nt(a, theirs).astype(BF16)
            net.send(f"{n}d{o % 2 or o}", n + "d", part.at[t, o], got.at[t, o], pair, "d")
            mine = g[xd * NC + core].reshape(NY * g.shape[2], g.shape[3])
            own[t, o] = nt(a, mine)
            work(0.4)

        def out_far():
            net.take(n + "d2", got.at[t, 2])
            far[t] = (own[t, 2] + got[t, 2].astype(F32)).astype(BF16)
            work(0.1)
            net.send(n + "f", n + "f", far.at[t, pl.ds(0, half_rows)], relay.at[t, 0], xup, "x+")
            net.send(n + "f", n + "f", far.at[t, pl.ds(half_rows, half_rows)], relay.at[t, 1], xdn, "x-")

        def out_near():
            net.take(n + "d1", got.at[t, pl.ds(0, 2)])
            near[t, 0, low, :] = (own[t, 1, low, :] + got[t, 1, low, :].astype(F32)).astype(BF16)
            near[t, 1, top, :] = (own[t, 3, top, :] + got[t, 3, top, :].astype(F32)).astype(BF16)
            work(0.1)
            at = pl.ds(half_rows, half_rows)
            net.send(n + "e", n + "e", near.at[t, 0, at], fin.at[t, 0, at], xup, "x+")
            at = pl.ds(0, half_rows)
            net.send(n + "e", n + "e", near.at[t, 1, at], fin.at[t, 1, at], xdn, "x-")

        def out_relay():
            net.take(n + "f", relay.at[t])
            near[t, 0, top, :] = (own[t, 1, top, :] + got[t, 1, top, :].astype(F32) + relay[t, 0].astype(F32)).astype(BF16)
            near[t, 1, low, :] = (own[t, 3, low, :] + got[t, 3, low, :].astype(F32) + relay[t, 1].astype(F32)).astype(BF16)
            work(0.1)
            at = pl.ds(0, half_rows)
            net.send(n + "e", n + "e", near.at[t, 0, at], fin.at[t, 0, at], xup, "x+")
            at = pl.ds(half_rows, half_rows)
            net.send(n + "e", n + "e", near.at[t, 1, at], fin.at[t, 1, at], xdn, "x-")

        def end():
            net.take(n + "d0", got.at[t, 0])
            net.take(n + "e", fin.at[t])
            finish(own[t, 0] + got[t, 0].astype(F32) + fin[t, 0].astype(F32) + fin[t, 1].astype(F32))

        ends.append((n + "d", part.at[t]))
        ends.append((n + "f", far.at[t]))
        ends.append((n + "e", near.at[t]))
        def mm_joint(o):
            a = lhs[...]
            xd = (x + o) % NX
            theirs = g[xd * NC + (1 - core)].reshape(NY * g.shape[2], g.shape[3])
            terms = nt(a, theirs).astype(BF16)
            for c in range(CHUNKS):
                part[c, o] = terms[c * span : (c + 1) * span]
                net.send(f"{n[0]}{c}d{o % 2 or o}", f"{n[0]}{c}d", part.at[c, o], got.at[c, o], pair, "d")
            mine = g[xd * NC + core].reshape(NY * g.shape[2], g.shape[3])
            terms = nt(a, mine)
            for c in range(CHUNKS):
                own[c, o] = terms[c * span : (c + 1) * span]
            work(0.4 + g.shape[3] / 1024)

        m = n[0] + "m" if joint else n + "m"
        if not joint or t == 0:
            for o in (2, 1, 3, 0):
                item(f"{m}{o}", deps, o)(mm_joint if joint else mm)
        item(n + "f", [m + "2"])(out_far)
        item(n + "n", [m + "1", m + "3"])(out_near)
        item(n + "r", [n + "f", n + "n"])(out_relay)
        item(n + "e", [n + "r", m + "0"])(end)

    share("s", s_all, 0, rows, [])
    for t in range(2):
        item(f"N{t}", ["s3", "L"], s_all, gain_r, t * rows // 2, rows // 2)(norm_rows)

    def weight(i, j=0, n=0):
        g = wholes[i]
        return g[:, :, :, j : j + (n or g.shape[3])].reshape(NZ * NY * g.shape[2], n or g.shape[3])

    def project_in():
        rec_in = nn(normed[...], weight(0)).astype(BF16)
        pad_r[0:8, :] = jnp.zeros((8, cols), F32)
        pad_r[8:, :] = rec_in.astype(F32)
        work(1.0)

    def project_gate():
        gate_src[...] = nn(normed[...], weight(1)).astype(BF16)
        work(1.0)

    item("P0", ["N0", "N1", "W0"])(project_in)
    item("P1", ["N0", "N1", "W1"])(project_gate)

    heads, block = rgm.shape[0], rgm.shape[1]

    def jump():
        wide_rows = jnp.concatenate([spike[...], jnp.zeros((8 - heads, rows), F32)], axis=0)
        jumpt[...] = wide_rows.T

    def settled():
        for copy in loads[7:]:
            copy.wait()

    item("L", [])(settled)
    item("J", ["L"])(jump)
    piece = 64

    def recur(r):
        base = GATE_POWER * softplus(-rate[...])
        lo = r * piece
        conv = rtaps[0:1, :] * pad_r[8 - 3 + lo : 8 - 3 + lo + piece, :]
        for k in range(1, 4):
            conv = conv + rtaps[k : k + 1, :] * pad_r[8 - 3 + k + lo : 8 - 3 + k + lo + piece, :]
        conv = conv.astype(BF16)
        reset, admit, jumps = [], [], []
        for h in range(heads):
            blk = conv[:, h * block : (h + 1) * block]
            reset.append(nn(blk, rgm[h]))
            admit.append(nn(blk, igm[h]))
            jumps.append(jnp.broadcast_to(jumpt[lo : lo + piece, h : h + 1], (piece, block)))
        reset = sigmoid(jnp.concatenate(reset, axis=1))
        admit = sigmoid(jnp.concatenate(admit, axis=1))
        log_decay = -reset * base + jnp.concatenate(jumps, axis=1)
        a = jnp.exp(log_decay)
        b = jnp.sqrt(one_minus_exp(2.0 * log_decay)) * admit * conv.astype(F32)
        row = lax.broadcasted_iota(jnp.int32, (piece, cols), 0)
        d = 1
        while d < piece:
            if d < 8:
                keep = row >= d
                pa = jnp.where(keep, pltpu.roll(a, d, 0), 1.0)
                pb = jnp.where(keep, pltpu.roll(b, d, 0), 0.0)
            else:
                pa = jnp.concatenate([jnp.ones((d, cols), F32), a[: piece - d]], axis=0)
                pb = jnp.concatenate([jnp.zeros((d, cols), F32), b[: piece - d]], axis=0)
            b = a * pb + b
            a = a * pa
            d *= 2
        states = b if r == 0 else a * carry[0:1, :] + b
        carry[0:1, :] = states[piece - 1 : piece, :]
        mixed[lo : lo + piece, :] = (states * gelu(gate_src[lo : lo + piece, :].astype(F32))).astype(BF16)
        work(0.7)

    per = span // piece
    for r in range(rows // piece):
        item(f"R{r}", ["P0", "P1", "J"] + ([f"R{r - 1}"] if r else []), r)(recur)

    def to_middle(t, total):
        at = slice(t * span, (t + 1) * span)
        m_all[tp, at, :] = (s_all[tp, at, :].astype(F32) + total.astype(BF16).astype(F32)).astype(BF16)
        work(0.15)

    for t in range(CHUNKS):
        scatter(
            f"a{t}", t, mixed, 2, own_a, part_a, got_a, far_a, near_a, relay_a, fin_a,
            ["W2"] + [f"R{q}" for q in range(rows // piece)], functools.partial(to_middle, t), True,
        )
        share(f"m{t}", m_all, t * span, span, [f"a{t}e"])
        item(f"M{t}", [f"m{t}3", "P0", "P1"], m_all, gain_f, t * span, span)(norm_rows)

    wide = g_fg.shape[3]

    def up(i, pad, j):
        pad[0:8, j : j + 256] = jnp.zeros((8, 256), F32)
        pad[8:, j : j + 256] = nn(normed[...], weight(i, j, 256)).astype(BF16).astype(F32)
        work(0.95)

    def mix(r):
        lo = r * piece
        gate = gtaps[0:1, :] * pad_g[6 + lo : 6 + lo + piece, :]
        value = vtaps[0:1, :] * pad_v[6 + lo : 6 + lo + piece, :]
        for k in range(1, 3):
            gate = gate + gtaps[k : k + 1, :] * pad_g[6 + k + lo : 6 + k + lo + piece, :]
            value = value + vtaps[k : k + 1, :] * pad_v[6 + k + lo : 6 + k + lo + piece, :]
        hidden[lo : lo + piece, :] = (gelu(gate) * value).astype(BF16)
        work(0.3)

    def to_final(t, total):
        at = slice(t * span, (t + 1) * span)
        last = m_all[tp, at, :].astype(F32) + total.astype(BF16).astype(F32)
        final[at, :] = last
        squares = last * last
        lanes = squares[:, 0:128] + squares[:, 128:256]
        sums = jnp.sum(lanes.T, axis=0, keepdims=True)
        stats[t, tp] = jnp.broadcast_to(sums, (8, span))
        work(0.5)
        for device in others:
            net.send(f"q{t}", f"q{t}", stats.at[t, tp], stats.at[t, tp], device, "s")

    def finish(t):
        net.take(f"q{t}", stats.at[t, pl.ds(0, 7)])
        at = slice(t * span, (t + 1) * span)
        total = stats[t, 0]
        for k in range(1, NX * NC):
            total = total + stats[t, k]
        inverse = lax.rsqrt(total * (1.0 / (cols * NX * NC)) + EPS).T[:, 0:1]
        gain = gain_c[:, pl.ds(pl.multiple_of(tp * cols, cols), cols)]
        out[at, :] = (final[at, :] * inverse * gain).astype(BF16)
        work(0.4)

    ups = []
    for i, pad in ((3, pad_g), (4, pad_v)):
        for j in range(0, wide, 256):
            ups.append(f"u{i}{j // 256}")
            item(ups[-1], [f"M{t}" for t in range(CHUNKS)] + [f"W{i}"], i, pad, j)(up)
    for t in range(CHUNKS):
        for q in range(per):
            r = t * per + q
            item(f"H{r}", ups + ([f"H{r - 1}"] if r else []), r)(mix)
        scatter(
            f"b{t}", t, hidden, 5, own_b, part_b, got_b, far_b, near_b, relay_b, fin_b,
            ["W5"] + [f"H{q}" for q in range(rows // piece)], functools.partial(to_final, t), True,
        )
        ends.append((f"q{t}", stats.at[t, pl.ds(0, 7)]))
        item(f"F{t}", [f"b{t}e"])(functools.partial(finish, t))

    emitted = set()

    def emit(name):
        if name in emitted:
            return
        deps, fn = items[name]
        for dep in deps:
            emit(dep)
        LOG.append(("item", name, deps))
        with scope(name):
            fn()
        emitted.add(name)

    names = tuple(items)
    for k in ORDER:
        emit(names[k])
    for name in names:
        emit(name)
    LOG.append(("names", names))
    LOG.append(("item", "drain", tuple(items)))
    with scope("drain"):
        for leave, ref in ends:
            net.left(leave, ref)
    assert not net.departures and set(net.arrivals) == net.taken, "unbalanced"
    LOG.append(("counts", len(net.arrivals), len(ends)))


def shards(
    stream, recurrence_input_weight, output_gate_weight, recurrence_gate_matrix, input_gate_matrix,
    channel_decay_rate, recurrence_taps, spike_log_decay, recurrence_output_weight, feedforward_gate_upward,
    feedforward_value_upward, feedforward_gate_taps, feedforward_value_taps, feedforward_down_weight,
    recurrence_norm_gain, feedforward_norm_gain, closing_norm_gain,
):
    rows, cols = stream.shape
    tps = NX * NC
    weights = (
        recurrence_input_weight, output_gate_weight, recurrence_output_weight.T,
        feedforward_gate_upward, feedforward_value_upward, feedforward_down_weight.T,
    )
    wide = feedforward_gate_upward.shape[1]
    hbm = pl.BlockSpec(memory_space=pltpu.MemorySpace.HBM)
    vmem = pl.BlockSpec(memory_space=pltpu.VMEM)
    small = (
        recurrence_gate_matrix, input_gate_matrix, channel_decay_rate.reshape(1, -1), recurrence_taps,
        spike_log_decay.T, feedforward_gate_taps, feedforward_value_taps,
        recurrence_norm_gain.reshape(1, -1), feedforward_norm_gain.reshape(1, -1), closing_norm_gain.reshape(1, -1),
    )
    span = rows // CHUNKS
    scatter = [
        pltpu.VMEM((CHUNKS, NX, span, cols), F32),
        pltpu.VMEM((CHUNKS, NX, span, cols), BF16),
        pltpu.VMEM((CHUNKS, NX, span, cols), BF16),
        pltpu.VMEM((CHUNKS, span, cols), BF16),
        pltpu.VMEM((CHUNKS, 2, span, cols), BF16),
        pltpu.VMEM((CHUNKS, 2, span // 2, cols), BF16),
        pltpu.VMEM((CHUNKS, 2, span, cols), BF16),
    ]
    return pl.pallas_call(
        layer_kernel,
        out_shape=jax.ShapeDtypeStruct((rows, cols), BF16),
        in_specs=[hbm] * 17,
        out_specs=vmem,
        scratch_shapes=[pltpu.VMEM((NZ, NY, *w.shape), BF16) for w in weights]
        + [
            pltpu.VMEM((tps, rows, cols), BF16),
            pltpu.VMEM((tps, rows, cols), BF16),
            pltpu.VMEM((rows, tps * cols), BF16),
            pltpu.VMEM((rows + 8, cols), F32),
            pltpu.VMEM((rows, cols), BF16),
            pltpu.VMEM((rows, cols), BF16),
            pltpu.VMEM((rows + 8, wide), F32),
            pltpu.VMEM((rows + 8, wide), F32),
            pltpu.VMEM((rows, wide), BF16),
            pltpu.VMEM((8, cols), F32),
        ]
        + scatter + scatter
        + [
            pltpu.VMEM((rows, cols), F32),
            pltpu.VMEM((CHUNKS, tps, 8, span), F32),
            pltpu.VMEM((rows, 8), F32),
        ]
        + [pltpu.VMEM(v.shape, v.dtype) for v in small]
        + [
            pltpu.SemaphoreType.DMA((32,)),
            pltpu.SemaphoreType.DMA((SEMS,)),
            pltpu.SemaphoreType.DMA((17,)),
        ],
        compiler_params=pltpu.CompilerParams(
            collective_id=0, has_side_effects=True, vmem_limit_bytes=60 * 1024 * 1024
        ),
        name="layer",
    )(
        stream, *weights, *small,
    )


def solution(mesh):
    in_specs = (
        P(("rep", "fs"), "tp"), P("fs", "tp"), P("fs", "tp"), P("tp", None, None), P("tp", None, None), P("tp"),
        P(None, "tp"), P(("rep", "fs"), "tp"), P("tp", "fs"), P("fs", "tp"), P("fs", "tp"), P(None, "tp"),
        P(None, "tp"), P("tp", "fs"), P(), P(), P(),
    )
    return jax.shard_map(
        shards, mesh=mesh, in_specs=in_specs, out_specs=P(("rep", "fs"), "tp"), check_vma=False
    )
```
